32 devices in a mesh: dp: 4 (over y, x), kv: 4 (over z), tp: 2 (over core).
Axes of the slice: x: 2, y: 2, z: 4, core: 2. Of those that a mesh axis runs over, the one named last changes fastest.
Arguments:
- piece_rows: bfloat16 [256, 2048], P(('dp', 'kv')), parts along dimension 0, may hold values from -6 to 6
- decode_rows: bfloat16 [16, 2048], P(('dp', 'kv')), parts along dimension 0, may hold values from -6 to 6
- prompt_latent: bfloat16 [4096, 512], P(('dp', 'kv')), parts along dimension 0, may hold values from -512 to 512
- prompt_rope_key: bfloat16 [4096, 32], P(('dp', 'kv')), parts along dimension 0, may hold values from -6 to 6
- decode_latent: bfloat16 [16, 512, 512], P(('dp', 'kv')), parts along dimension 0, may hold values from -512 to 512
- decode_rope_key: bfloat16 [16, 512, 32], P(('dp', 'kv')), parts along dimension 0, may hold values from -6 to 6
- dec_lengths: int32 [16], P(('dp', 'kv')), parts along dimension 0, may hold values from 1 to 512, as said below
- w_qdown: bfloat16 [2048, 512], replicated, may hold values from -0.125 to 0.125
- q_gain: float32 [512], replicated, may hold values from 0.1 to 1.9
- w_qup: bfloat16 [512, 16, 96], P(None, 'tp'), may hold values from -0.25 to 0.25
- w_kvdown: bfloat16 [2048, 512], replicated, may hold values from -0.125 to 0.125
- w_krope: bfloat16 [2048, 32], replicated, may hold values from -0.125 to 0.125
- kv_gain: float32 [512], replicated, may hold values from 0.1 to 1.9
- w_kup: bfloat16 [512, 16, 64], P(None, 'tp'), may hold values from -0.25 to 0.25
- w_vup: bfloat16 [512, 16, 64], P(None, 'tp'), may hold values from -0.25 to 0.25
- w_out: bfloat16 [16, 64, 2048], P('tp'), may hold values from -0.1875 to 0.1875
Outputs:
- piece_out: bfloat16 [256, 2048], P(('dp', 'kv')), parts along dimension 0
- decode_out: bfloat16 [16, 2048], P(('dp', 'kv')), parts along dimension 0
- piece_latent: bfloat16 [256, 512], P(('dp', 'kv')), parts along dimension 0
- piece_rope: bfloat16 [256, 32], P(('dp', 'kv')), parts along dimension 0
- decode_new_latent: bfloat16 [16, 512], P(('dp', 'kv')), parts along dimension 0
- decode_new_rope: bfloat16 [16, 32], P(('dp', 'kv')), parts along dimension 0
The draws below stay inside these ranges and needn't reach their ends.
There are 4 independent parts, one for each index of `dp`. The reference program is written for one: setup_inputs(seed, part) draws one part's arguments, and reference() takes and returns one part's arrays. A program takes and returns all parts, laid end to end along the dimension named above; an argument that names none is the same for every part. Nothing has to cross between parts.
Inputs may be any that keep to these rules, and one draw needn't show every extreme that they name: `dec_lengths`: each group of requests has some decoding sequence with exactly 512 cached rows.
All inputs are finite; a program needn't handle non-finite values.
Results may differ from the reference program's by a relative error of at most 0.03.
Values may be sent and summed in bfloat16 or wider, within the bound.
No kernel may reach another device: no remote copies, remote signals or barrier semaphores. Data moves between devices by JAX's collectives and lax.ppermute only.
A program may use at most 64 MiB of HBM per device.

```python
import jax
import jax.numpy as jnp
from jax import lax

D_MODEL = 2048
HEADS = 16
NOPE_DIM = 64
ROPE_DIM = 32
VALUE_DIM = 64
Q_LATENT = 512
KV_LATENT = 512
PIECE_DEV = 16
CACHE_DEV = 256
DEC_CACHE = 512
PIECE = 64
CONTEXT = 1024
DECODES = 4
N_KV = 4
N_TP = 2


def draw_dec_lengths(key, part):
    lengths = jax.random.randint(key, (DECODES,), 1, DEC_CACHE + 1)
    chosen = jax.random.randint(jax.random.fold_in(key, 7), (), 0, DECODES)
    return jnp.where(jnp.arange(DECODES) == chosen, DEC_CACHE, lengths).astype(jnp.int32)


def draw_prompt_latent(key, part):
    base = jax.random.truncated_normal(jax.random.fold_in(key, 211), -6.0, 6.0, (CONTEXT, KV_LATENT), jnp.float32)
    return base.astype(jnp.bfloat16)


def draw_decode_latent(key, part):
    base = jax.random.truncated_normal(jax.random.fold_in(key, 221), -6.0, 6.0, (DECODES * DEC_CACHE, KV_LATENT), jnp.float32)
    return base.reshape(DECODES, DEC_CACHE, KV_LATENT).astype(jnp.bfloat16)


def block_levels(stream_key, shape, shards, least, high):
    level, own = 1.0, jax.random.fold_in(stream_key, 6)
    for dim, blocks in shards:
        draws = jnp.exp(jax.random.uniform(jax.random.fold_in(own, dim), (blocks,), jnp.float32, least / len(shards), high / len(shards)))
        level = level * jnp.repeat(draws, shape[dim] // blocks).reshape([-1 if axis == dim else 1 for axis in range(len(shape))])
    return level


def bell_draw(stream_key, shape, spread, reach, shards=(), held_as=jnp.bfloat16):
    factor_of = block_levels(stream_key, shape, shards, -0.22, 0.18) if shards else 1.0
    drawn = jax.random.normal(stream_key, shape, jnp.float32) * spread * factor_of
    return jnp.minimum(jnp.maximum(drawn, -reach), reach).astype(held_as)


def setup_inputs(seed: int = 0, part: int = 0) -> dict:
    key_of = jax.random.split(jax.random.key(seed), 17)
    part_keys = jax.random.split(jax.random.fold_in(key_of[16], part), 17)
    piece_rows = bell_draw(part_keys[0], (PIECE, D_MODEL), 1.0, 6.0, ((0, 4),))
    decode_rows = bell_draw(part_keys[1], (DECODES, D_MODEL), 1.0, 6.0, ((0, 4),))
    prompt_latent = draw_prompt_latent(jax.random.fold_in(jax.random.fold_in(key_of[16], part), 71), part)
    prompt_rope_key = bell_draw(part_keys[3], (CONTEXT, ROPE_DIM), 1.0, 6.0, ((0, 4),))
    decode_latent = draw_decode_latent(jax.random.fold_in(jax.random.fold_in(key_of[16], part), 71), part)
    decode_rope_key = bell_draw(part_keys[5], (DECODES, DEC_CACHE, ROPE_DIM), 1.0, 6.0, ((0, 4),))
    dec_lengths = draw_dec_lengths(jax.random.fold_in(jax.random.fold_in(key_of[16], part), 71), part)
    w_qdown = bell_draw(key_of[7], (D_MODEL, Q_LATENT), D_MODEL ** -0.5, 0.125)
    q_gain = jnp.clip(1.0 + 0.18 * jax.random.normal(key_of[8], (Q_LATENT,), jnp.float32), 0.1, 1.9)
    w_qup = bell_draw(key_of[9], (Q_LATENT, HEADS, NOPE_DIM + ROPE_DIM), Q_LATENT ** -0.5, 0.25, ((1, 2),))
    w_kvdown = bell_draw(key_of[10], (D_MODEL, KV_LATENT), D_MODEL ** -0.5, 0.125)
    w_krope = bell_draw(key_of[11], (D_MODEL, ROPE_DIM), D_MODEL ** -0.5, 0.125)
    kv_gain = jnp.clip(1.0 + 0.18 * jax.random.normal(key_of[12], (KV_LATENT,), jnp.float32), 0.1, 1.9)
    w_kup = bell_draw(key_of[13], (KV_LATENT, HEADS, NOPE_DIM), KV_LATENT ** -0.5, 0.25, ((1, 2),))
    w_vup = bell_draw(key_of[14], (KV_LATENT, HEADS, VALUE_DIM), KV_LATENT ** -0.5, 0.25, ((1, 2),))
    w_out = bell_draw(key_of[15], (HEADS, VALUE_DIM, D_MODEL), (HEADS * VALUE_DIM) ** -0.5, 0.1875, ((0, 2),))
    return dict(piece_rows=piece_rows, decode_rows=decode_rows, prompt_latent=prompt_latent, prompt_rope_key=prompt_rope_key, decode_latent=decode_latent, decode_rope_key=decode_rope_key, dec_lengths=dec_lengths, w_qdown=w_qdown, q_gain=q_gain, w_qup=w_qup, w_kvdown=w_kvdown, w_krope=w_krope, kv_gain=kv_gain, w_kup=w_kup, w_vup=w_vup, w_out=w_out)


def rms_scale(values, gain):
    return values * lax.rsqrt(lax.optimization_barrier(jnp.mean(values * values, axis=-1, keepdims=True)) + 1e-06) * gain

def rotate(values, positions):
    half = values.shape[-1] // 2
    inverse = jnp.power(10000.0, -jnp.arange(half, dtype=jnp.float32) * 2.0 / values.shape[-1])
    angle = positions.astype(jnp.float32)[:, None] * inverse[None, :]
    angle = angle.reshape((positions.shape[0],) + (1,) * (values.ndim - 2) + (half,))
    cosine, sine = (jnp.cos(angle), jnp.sin(angle))
    first, second = (values[..., :half], values[..., half:])
    return jnp.concatenate([first * cosine - second * sine, second * cosine + first * sine], -1)

def project(rows, positions, w_qdown, q_gain, w_qup, w_kvdown, w_krope, kv_gain):
    query_latent = rms_scale(jnp.dot(rows, w_qdown, preferred_element_type=jnp.float32), q_gain).astype(jnp.bfloat16)
    full = jnp.einsum('rq,qhe->rhe', query_latent.astype(jnp.float32), w_qup.astype(jnp.float32))
    query_nope = full[..., :NOPE_DIM].astype(jnp.bfloat16)
    query_rope = rotate(full[..., NOPE_DIM:], positions).astype(jnp.bfloat16)
    latent = rms_scale(jnp.dot(rows, w_kvdown, preferred_element_type=jnp.float32), kv_gain).astype(jnp.bfloat16)
    rope_key = rotate(jnp.dot(rows, w_krope, preferred_element_type=jnp.float32), positions).astype(jnp.bfloat16)
    return (query_nope, query_rope, latent, rope_key)

def out_project(heads, w_out):
    groups = heads.reshape(heads.shape[0], N_TP, HEADS // N_TP, VALUE_DIM).astype(jnp.float32)
    weights = w_out.reshape(N_TP, HEADS // N_TP, VALUE_DIM, D_MODEL).astype(jnp.float32)
    terms = jnp.einsum('rghv,ghvd->grd', groups, weights).astype(jnp.bfloat16).astype(jnp.float32)
    return lax.optimization_barrier(jnp.sum(terms, axis=0)).astype(jnp.bfloat16)

def reference(piece_rows, decode_rows, prompt_latent, prompt_rope_key, decode_latent, decode_rope_key, dec_lengths, w_qdown, q_gain, w_qup, w_kvdown, w_krope, kv_gain, w_kup, w_vup, w_out):
    scale = (NOPE_DIM + ROPE_DIM) ** (-0.5)
    piece_pos = CONTEXT + jnp.arange(PIECE, dtype=jnp.int32)
    piece_nope, piece_qrope, piece_latent, piece_rope = project(piece_rows, piece_pos, w_qdown, q_gain, w_qup, w_kvdown, w_krope, kv_gain)
    dec_nope, dec_qrope, dec_latent, dec_rope = project(decode_rows, dec_lengths, w_qdown, q_gain, w_qup, w_kvdown, w_krope, kv_gain)

    def span(index):
        lat = jnp.concatenate([lax.dynamic_slice_in_dim(prompt_latent, index * CACHE_DEV, CACHE_DEV, 0), lax.dynamic_slice_in_dim(piece_latent, index * PIECE_DEV, PIECE_DEV, 0)], 0)
        keyrot = jnp.concatenate([lax.dynamic_slice_in_dim(prompt_rope_key, index * CACHE_DEV, CACHE_DEV, 0), lax.dynamic_slice_in_dim(piece_rope, index * PIECE_DEV, PIECE_DEV, 0)], 0)
        key_pos = jnp.concatenate([index * CACHE_DEV + jnp.arange(CACHE_DEV, dtype=jnp.int32), CONTEXT + index * PIECE_DEV + jnp.arange(PIECE_DEV, dtype=jnp.int32)])
        key_nope = jnp.einsum('sl,lhe->she', lat.astype(jnp.float32), w_kup.astype(jnp.float32)).astype(jnp.bfloat16)
        values = jnp.einsum('sl,lhe->she', lat.astype(jnp.float32), w_vup.astype(jnp.float32)).astype(jnp.bfloat16)
        scores = (jnp.einsum('qhe,she->qhs', piece_nope.astype(jnp.float32), key_nope.astype(jnp.float32)) + jnp.einsum('qhe,se->qhs', piece_qrope.astype(jnp.float32), keyrot.astype(jnp.float32))) * scale
        allowed = key_pos[None, None, :] <= piece_pos[:, None, None]
        scores = jnp.where(allowed, scores, -1e+30)
        top = lax.optimization_barrier(jnp.max(scores, axis=-1))
        weights = jnp.exp(scores - top[..., None])
        total = lax.optimization_barrier(jnp.sum(weights, axis=-1))
        part = jnp.einsum('qhs,she->qhe', weights.astype(jnp.bfloat16).astype(jnp.float32), values.astype(jnp.float32))
        return (part.astype(jnp.bfloat16), top, total)
    parts, tops, totals = lax.map(span, jnp.arange(N_KV, dtype=jnp.int32))
    best = lax.optimization_barrier(jnp.max(tops, axis=0))
    factors = jnp.exp(tops - best[None])
    denom = lax.optimization_barrier(jnp.sum(totals * factors, axis=0))
    piece_heads = (lax.optimization_barrier(jnp.sum(parts.astype(jnp.float32) * factors[..., None], axis=0)) / denom[..., None]).astype(jnp.bfloat16)
    absorbed = jnp.einsum('bhe,lhe->bhl', dec_nope.astype(jnp.float32), w_kup.astype(jnp.float32)).astype(jnp.bfloat16)
    abs32 = absorbed.astype(jnp.float32)
    cached = (jnp.einsum('bhl,bcl->bhc', abs32, decode_latent.astype(jnp.float32)) + jnp.einsum('bhe,bce->bhc', dec_qrope.astype(jnp.float32), decode_rope_key.astype(jnp.float32))) * scale
    valid = jnp.arange(DEC_CACHE, dtype=jnp.int32)[None, None, :] < dec_lengths[:, None, None]
    cached = jnp.where(valid, cached, -1e+30)
    own = (jnp.einsum('bhl,bl->bh', abs32, dec_latent.astype(jnp.float32)) + jnp.einsum('bhe,be->bh', dec_qrope.astype(jnp.float32), dec_rope.astype(jnp.float32))) * scale
    top = jnp.maximum(lax.optimization_barrier(jnp.max(cached, axis=-1)), own)
    cached_w = jnp.exp(cached - top[..., None])
    own_w = jnp.exp(own - top)
    denom = lax.optimization_barrier(jnp.sum(cached_w, axis=-1)) + own_w
    cached_p = (cached_w / denom[..., None]).astype(jnp.bfloat16).astype(jnp.float32)
    own_p = (own_w / denom).astype(jnp.bfloat16).astype(jnp.float32)
    context = (jnp.einsum('bhc,bcl->bhl', cached_p, decode_latent.astype(jnp.float32)) + own_p[..., None] * dec_latent.astype(jnp.float32)[:, None, :]).astype(jnp.bfloat16)
    decode_heads = jnp.einsum('bhl,lhv->bhv', context.astype(jnp.float32), w_vup.astype(jnp.float32)).astype(jnp.bfloat16)
    piece_out = out_project(piece_heads, w_out)
    decode_out = out_project(decode_heads, w_out)
    return (piece_out, decode_out, piece_latent, piece_rope, dec_latent, dec_rope)
```

```python
import jax
import jax.numpy as jnp
from jax import lax
from jax.sharding import PartitionSpec as P

NOPE_DIM = 64
ROPE_DIM = 32
MAX_PERMUTES = 8


def rms_scale(values, gain):
    return values * lax.rsqrt(jnp.mean(values * values, axis=-1, keepdims=True) + 1e-06) * gain


def rotate(values, positions):
    half = values.shape[-1] // 2
    inverse = jnp.power(10000.0, -jnp.arange(half, dtype=jnp.float32) * 2.0 / values.shape[-1])
    angle = positions.astype(jnp.float32)[:, None] * inverse[None, :]
    angle = angle.reshape((positions.shape[0],) + (1,) * (values.ndim - 2) + (half,))
    cosine, sine = (jnp.cos(angle), jnp.sin(angle))
    first, second = (values[..., :half], values[..., half:])
    return jnp.concatenate([first * cosine - second * sine, second * cosine + first * sine], -1)


def query_heads(latent_rows, w_qup, positions):
    full = jnp.einsum("rq,qhe->rhe", latent_rows, w_qup, preferred_element_type=jnp.float32)
    nope = full[..., :NOPE_DIM].astype(jnp.bfloat16)
    turned = rotate(full[..., NOPE_DIM:], positions).astype(jnp.bfloat16)
    return (nope, turned)


def shift(values, axis, step):
    size = lax.axis_size(axis)
    return lax.ppermute(values, axis, [(i, (i + step) % size) for i in range(size)])


def gather_blocks(values, axis):
    size = lax.axis_size(axis)
    if size > MAX_PERMUTES:
        blocks = lax.all_gather(values, axis, axis=0)
        return jnp.roll(jnp.flip(blocks, 0), lax.axis_index(axis) + 1, axis=0)
    return jnp.stack([values] + [shift(values, axis, s) for s in range(1, size)])


def return_blocks(blocks, axis):
    size = lax.axis_size(axis)
    if size > MAX_PERMUTES:
        ordered = jnp.flip(jnp.roll(blocks, -lax.axis_index(axis) - 1, axis=0), 0)
        return lax.all_to_all(ordered, axis, split_axis=0, concat_axis=0, tiled=True)
    return jnp.stack([blocks[0]] + [shift(blocks[s], axis, size - s) for s in range(1, size)])


def split3(values):
    high = lax.reduce_precision(values, 8, 7)
    rest = values - high
    middle = lax.reduce_precision(rest, 8, 7)
    return [piece.astype(jnp.bfloat16) for piece in (high, middle, rest - middle)]


def decode_attend(
    dec_nope,
    dec_qrope,
    dec_latent,
    dec_rope,
    decode_latent,
    decode_rope_key,
    dec_lengths,
    w_kup,
    w_vup,
    scale,
):
    absorbed = jnp.einsum(
        "bhe,lhe->bhl", dec_nope, w_kup, preferred_element_type=jnp.float32
    ).astype(jnp.bfloat16)
    cached = (
        jnp.einsum("bhl,bcl->bhc", absorbed, decode_latent, preferred_element_type=jnp.float32)
        + jnp.einsum("bhe,bce->bhc", dec_qrope, decode_rope_key, preferred_element_type=jnp.float32)
    ) * scale
    valid = (
        jnp.arange(decode_latent.shape[1], dtype=jnp.int32)[None, None, :]
        < dec_lengths[:, None, None]
    )
    cached = jnp.where(valid, cached, -1e30)
    own = (
        jnp.einsum("bhl,bl->bh", absorbed, dec_latent, preferred_element_type=jnp.float32)
        + jnp.einsum("bhe,be->bh", dec_qrope, dec_rope, preferred_element_type=jnp.float32)
    ) * scale
    top = jnp.maximum(jnp.max(cached, axis=-1), own)
    cached_w = jnp.exp(cached - top[..., None])
    own_w = jnp.exp(own - top)
    denom = jnp.sum(cached_w, axis=-1) + own_w
    cached_p = (cached_w / denom[..., None]).astype(jnp.bfloat16)
    own_p = (own_w / denom).astype(jnp.bfloat16).astype(jnp.float32)
    context = (
        jnp.einsum("bhc,bcl->bhl", cached_p, decode_latent, preferred_element_type=jnp.float32)
        + own_p[..., None] * dec_latent.astype(jnp.float32)[:, None, :]
    ).astype(jnp.bfloat16)
    return jnp.einsum("bhl,lhv->bhv", context, w_vup, preferred_element_type=jnp.float32).astype(
        jnp.bfloat16
    )


def per_device(
    piece_rows,
    decode_rows,
    prompt_latent,
    prompt_rope_key,
    decode_latent,
    decode_rope_key,
    dec_lengths,
    w_qdown,
    q_gain,
    w_qup,
    w_kvdown,
    w_krope,
    kv_gain,
    w_kup,
    w_vup,
    w_out,
):
    scale = (NOPE_DIM + ROPE_DIM) ** (-0.5)
    shards = lax.axis_size("kv")
    index = lax.axis_index("kv")
    piece_dev = piece_rows.shape[0]
    cache_dev = prompt_latent.shape[0]
    context_len = cache_dev * shards
    rows = jnp.concatenate([piece_rows, decode_rows], 0)
    query_latent = rms_scale(
        jnp.dot(rows, w_qdown, preferred_element_type=jnp.float32), q_gain
    ).astype(jnp.bfloat16)
    block_rows = gather_blocks(query_latent[:piece_dev], "kv").reshape(-1, query_latent.shape[1])
    latent_new = rms_scale(
        jnp.dot(rows, w_kvdown, preferred_element_type=jnp.float32), kv_gain
    ).astype(jnp.bfloat16)
    offsets = jnp.arange(piece_dev, dtype=jnp.int32)
    piece_pos = context_len + index * piece_dev + offsets
    positions = jnp.concatenate([piece_pos, dec_lengths])
    rope_new = rotate(jnp.dot(rows, w_krope, preferred_element_type=jnp.float32), positions).astype(
        jnp.bfloat16
    )
    owners = (index - jnp.arange(shards, dtype=jnp.int32) + shards) % shards
    query_pos = (context_len + owners[:, None] * piece_dev + offsets[None, :]).reshape(-1)
    dec_nope, dec_qrope = query_heads(query_latent[piece_dev:], w_qup, dec_lengths)
    dec_latent = latent_new[piece_dev:]
    dec_rope = rope_new[piece_dev:]
    key_latent = jnp.concatenate([prompt_latent, latent_new[:piece_dev]], 0)
    key_turned = jnp.concatenate([prompt_rope_key, rope_new[:piece_dev]], 0)
    key_pos = jnp.concatenate(
        [index * cache_dev + jnp.arange(cache_dev, dtype=jnp.int32), piece_pos]
    )
    key_nope = jnp.einsum(
        "sl,lhe->she", key_latent, w_kup, preferred_element_type=jnp.float32
    ).astype(jnp.bfloat16)
    values = jnp.einsum(
        "sl,lhe->she", key_latent, w_vup, preferred_element_type=jnp.float32
    ).astype(jnp.bfloat16)
    nope, turned = query_heads(block_rows, w_qup, query_pos)
    scores = (
        jnp.einsum("qhe,she->qhs", nope, key_nope, preferred_element_type=jnp.float32)
        + jnp.einsum("qhe,se->qhs", turned, key_turned, preferred_element_type=jnp.float32)
    ) * scale
    scores = jnp.where(key_pos[None, None, :] <= query_pos[:, None, None], scores, -1e30)
    top = jnp.max(scores, axis=-1)
    weights = jnp.exp(scores - top[..., None])
    total = jnp.sum(weights, axis=-1)
    part = jnp.einsum(
        "qhs,she->qhe", weights.astype(jnp.bfloat16), values, preferred_element_type=jnp.float32
    )
    heads_dev, value_dim = part.shape[1:]
    width = heads_dev * value_dim
    packed = jnp.concatenate(
        [part.astype(jnp.bfloat16).reshape(-1, width)] + split3(top) + split3(total), -1
    ).reshape(shards, piece_dev, -1)
    got = return_blocks(packed, "kv")
    decode_heads = decode_attend(
        dec_nope,
        dec_qrope,
        dec_latent,
        dec_rope,
        decode_latent,
        decode_rope_key,
        dec_lengths,
        w_kup,
        w_vup,
        scale,
    )
    got_parts = got[..., :width].reshape(shards, piece_dev, heads_dev, value_dim)
    stats = got[..., width:].astype(jnp.float32).reshape(shards, piece_dev, 2, 3, heads_dev)
    stats = stats[..., 0, :] + stats[..., 1, :] + stats[..., 2, :]
    got_tops, got_totals = stats[:, :, 0], stats[:, :, 1]
    best = jnp.max(got_tops, axis=0)
    factors = jnp.exp(got_tops - best[None])
    denom = jnp.sum(got_totals * factors, axis=0)
    piece_heads = (
        jnp.sum(got_parts.astype(jnp.float32) * factors[..., None], axis=0) / denom[..., None]
    ).astype(jnp.bfloat16)
    all_heads = jnp.concatenate([piece_heads, decode_heads], 0)
    term = jnp.einsum("rhv,hvd->rd", all_heads, w_out, preferred_element_type=jnp.float32)
    term = term.astype(jnp.bfloat16)
    summed = term.astype(jnp.float32)
    for step in range(1, lax.axis_size("tp")):
        summed = summed + shift(term, "tp", step).astype(jnp.float32)
    summed = summed.astype(jnp.bfloat16)
    return (
        summed[:piece_dev],
        summed[piece_dev:],
        latent_new[:piece_dev],
        rope_new[:piece_dev],
        dec_latent,
        dec_rope,
    )


def solution(mesh):
    in_specs = (
        P(("dp", "kv"), None),
        P(("dp", "kv"), None),
        P(("dp", "kv"), None),
        P(("dp", "kv"), None),
        P(("dp", "kv"), None, None),
        P(("dp", "kv"), None, None),
        P(("dp", "kv")),
        P(),
        P(),
        P(None, "tp", None),
        P(),
        P(),
        P(),
        P(None, "tp", None),
        P(None, "tp", None),
        P("tp", None, None),
    )
    out_specs = (
        P(("dp", "kv"), None),
        P(("dp", "kv"), None),
        P(("dp", "kv"), None),
        P(("dp", "kv"), None),
        P(("dp", "kv"), None),
        P(("dp", "kv"), None),
    )
    return jax.shard_map(
        per_device, mesh=mesh, in_specs=in_specs, out_specs=out_specs, check_vma=False
    )
```

```python
import functools

import jax
import jax.numpy as jnp
import numpy as np
from jax import lax
from jax.experimental import pallas as pl
from jax.experimental.pallas import tpu as pltpu
from jax.sharding import PartitionSpec as P

LANES = 128
GROUP = 256
MAX_PERMUTES = 8
ROPE_BASE = 10000.0
VMEM = pl.BlockSpec(memory_space=pltpu.VMEM)
SMEM = pl.BlockSpec(memory_space=pltpu.SMEM)
HBM = pl.BlockSpec(memory_space=pltpu.HBM)
NT = (((1,), (1,)), ((), ()))
F32 = jnp.float32
BF16 = jnp.bfloat16


def dot(a, b):
    return jnp.dot(a, b, preferred_element_type=F32)


def dot_nt(a, b):
    return lax.dot_general(a, b, NT, preferred_element_type=F32)


def lane_index(shape):
    return lax.broadcasted_iota(jnp.int32, shape, len(shape) - 1)


def row_index(shape):
    return lax.broadcasted_iota(jnp.int32, shape, 0)


def rms_scale(values, gain):
    return values * lax.rsqrt(jnp.mean(values * values, axis=-1, keepdims=True) + 1e-06) * gain


def turn(values, cosine, signed_sine, rope):
    half = rope // 2
    swapped = jnp.where(
        lane_index(values.shape) % rope < half,
        pltpu.roll(values, LANES - half, 1),
        pltpu.roll(values, half, 1),
    )
    return values * cosine + swapped * signed_sine


def diagonal(values, count, width):
    owner = lane_index(values.shape) // width
    return jnp.concatenate([jnp.where(owner == j, values, 0.0) for j in range(count)], 0)


def spread_rows(row, rows):
    return jnp.broadcast_to(row.astype(F32), (rows, row.shape[1])).astype(row.dtype)


def query_latent_kernel(piece_ref, dec_ref, w_hbm, gain_ref, out_ref, dec_out_ref, w_ref, sems):
    chunks = sems.shape[0]
    depth = w_ref.shape[0] // chunks
    copies = []
    for c in range(chunks):
        part = pl.ds(c * depth, depth)
        copies.append(pltpu.make_async_copy(w_hbm.at[part], w_ref.at[part], sems.at[c]))
        copies[-1].start()
    piece = piece_ref[...]
    rows = jnp.concatenate([piece, spread_rows(dec_ref[...], piece.shape[0])], 0)
    total = jnp.zeros((rows.shape[0], w_ref.shape[1]), F32)
    for c in range(chunks):
        copies[c].wait()
        part = slice(c * depth, (c + 1) * depth)
        total = total + dot(rows[:, part], w_ref[part, :])
    latent = rms_scale(total, gain_ref[...]).astype(BF16)
    out_ref[...] = latent[: piece.shape[0]]
    dec_out_ref[...] = latent[piece.shape[0] :]


def keys_kernel(
    context,
    lengths_ref,
    piece_ref,
    dec_ref,
    w_ref,
    w_rope_ref,
    gain_ref,
    cos_ref,
    sin_ref,
    freq_ref,
    prompt_ref,
    w_kup_ref,
    w_vup_ref,
    latent_ref,
    dec_latent_ref,
    rope_ref,
    dec_rope_ref,
    key_ref,
    value_ref,
    new_key_ref,
    new_value_ref,
    new_rope_ref,
    dec_rows_ref,
    dec_rope_rows_ref,
):
    count = piece_ref.shape[0]
    rope = w_rope_ref.shape[0]
    piece = piece_ref[...]
    rows = jnp.concatenate([piece, spread_rows(dec_ref[...], count)], 0)
    latent = rms_scale(dot(rows, w_ref[...]), gain_ref[...]).astype(BF16)
    w_rope = jnp.concatenate([w_rope_ref[...]] * (LANES // rope), 0)
    raw = dot_nt(rows, w_rope)
    index = lax.axis_index("kv")
    own = pl.ds(pl.multiple_of(index * count, count), count)
    new_rope = turn(raw[:count], cos_ref[own, :], sin_ref[own, :], rope).astype(BF16)
    angle = lengths_ref[0].astype(F32) * freq_ref[...]
    sign = jnp.where(lane_index(angle.shape) % rope < rope // 2, -1.0, 1.0)
    dec_rope = turn(raw[count:], jnp.cos(angle), jnp.sin(angle) * sign, rope).astype(BF16)
    latent_ref[...] = latent[:count]
    dec_latent_ref[...] = latent[count : count + 1]
    rope_ref[...] = new_rope[:, :rope]
    dec_rope_ref[...] = dec_rope[:1, :rope]
    new_rope_ref[...] = new_rope
    dec_rows_ref[...] = latent[count:]
    dec_rope_rows_ref[...] = dec_rope
    w_kup, w_vup = w_kup_ref[...], w_vup_ref[...]
    prompt = prompt_ref[...]
    key_ref[...] = dot_nt(prompt, w_kup).astype(BF16)
    value_ref[...] = dot_nt(prompt, w_vup).astype(BF16)
    new_key_ref[...] = dot_nt(latent[:count], w_kup).astype(BF16)
    new_value_ref[...] = dot_nt(latent[:count], w_vup).astype(BF16)


def split_query_weights(w_ref, nope):
    heads = w_ref.shape[0]
    w_nope = jnp.concatenate([w_ref[h, :nope, :] for h in range(heads)], 0)
    w_rope = jnp.concatenate([w_ref[h, nope:, :] for h in range(heads)], 0)
    return w_nope, w_rope


def attend_kernel(relative, nope, *refs):
    (
        w_ref,
        key_ref,
        value_ref,
        new_key_ref,
        new_value_ref,
        new_rope_ref,
        rope_ref,
        cos_ref,
        sin_ref,
    ) = refs[:9]
    latent_refs, out_ref = refs[9:-1], refs[-1]
    shards = lax.axis_size("kv")
    index = lax.axis_index("kv")
    heads = w_ref.shape[0]
    rope = w_ref.shape[1] - nope
    count = new_key_ref.shape[0]
    latents = jnp.concatenate([ref[...] for ref in latent_refs], 0)
    queries = latents.shape[0]
    blocks = queries // count
    first = 0 if relative else pl.program_id(0) * blocks
    owners = []
    for s in range(blocks):
        owners.append(lax.rem(index - s + shards, shards) if relative else first + s)
    tables = [pl.ds(pl.multiple_of(owner * count, count), count) for owner in owners]
    cosine = jnp.concatenate([cos_ref[part, :] for part in tables], 0)
    sine = jnp.concatenate([sin_ref[part, :] for part in tables], 0)
    scale = (nope + rope) ** (-0.5)
    w_nope, w_rope = split_query_weights(w_ref, nope)
    q_nope = dot_nt(latents, w_nope).astype(BF16).astype(F32)
    q_rope = dot_nt(latents, w_rope)
    per = GROUP // nope
    rope_keys = jnp.concatenate([rope_ref[...]] * (LANES // rope), 0)
    new_rope = new_rope_ref[...]
    row = row_index((count, count))
    column = lane_index((count, count))
    allowed = jnp.concatenate(
        [index * count + column <= owner * count + row for owner in owners] * per, 0
    )
    lane = lane_index((queries, LANES))
    stats = jnp.zeros((queries, LANES), F32)
    for g in range(heads // per):
        wide = slice(g * GROUP, (g + 1) * GROUP)
        turned = turn(q_rope[:, g * LANES : (g + 1) * LANES], cosine, sine, rope)
        spread = diagonal(q_nope[:, wide], per, nope).astype(BF16)
        spread_rope = diagonal(turned, per, rope).astype(BF16)
        old = (dot_nt(spread, key_ref[:, wide]) + dot(spread_rope, rope_keys)) * scale
        new = (dot_nt(spread, new_key_ref[:, wide]) + dot_nt(spread_rope, new_rope)) * scale
        new = jnp.where(allowed, new, -1e30)
        top = jnp.maximum(
            jnp.max(old, axis=-1, keepdims=True), jnp.max(new, axis=-1, keepdims=True)
        )
        old = jnp.exp(old - top)
        new = jnp.exp(new - top)
        total = jnp.sum(old, axis=-1, keepdims=True) + jnp.sum(new, axis=-1, keepdims=True)
        mixed = dot(old.astype(BF16), value_ref[:, wide]) + dot(
            new.astype(BF16), new_value_ref[:, wide]
        )
        owner_lane = lane_index((queries, GROUP)) // nope
        part = jnp.zeros((queries, GROUP), F32)
        for j in range(per):
            own = slice(j * queries, (j + 1) * queries)
            part = jnp.where(owner_lane == j, mixed[own], part)
            h = g * per + j
            stats = jnp.where(
                lane % heads == h, jnp.where(lane < 3 * heads, top[own], total[own]), stats
            )
        out_ref[:, wide] = part.astype(BF16)
    high = stats.astype(BF16).astype(F32)
    rest = stats - high
    middle = rest.astype(BF16).astype(F32)
    piece = (lane // heads) % 3
    stats = jnp.where(piece == 0, high, jnp.where(piece == 1, middle, rest - middle))
    stats = jnp.where(lane < 6 * heads, stats, 0.0)
    out_ref[:, heads * nope :] = stats.astype(BF16)


def decode_kernel(
    nope,
    lengths_ref,
    q_ref,
    w_ref,
    w_kup_ref,
    w_vup_ref,
    latent_ref,
    rope_ref,
    new_latent_ref,
    new_rope_ref,
    freq_ref,
    out_ref,
):
    heads = w_ref.shape[0]
    rope = w_ref.shape[1] - nope
    length = lengths_ref[0]
    scale = (nope + rope) ** (-0.5)
    latents = q_ref[...]
    rows = latents.shape[0]
    w_nope, w_rope = split_query_weights(w_ref, nope)
    q_nope = dot_nt(latents, w_nope)
    q_rope = dot_nt(latents, w_rope)
    angle = length.astype(F32) * freq_ref[...]
    sign = jnp.where(lane_index(angle.shape) % rope < rope // 2, -1.0, 1.0)
    cosine, sine = jnp.cos(angle), jnp.sin(angle) * sign
    shape = q_nope.shape
    spread = jnp.where(lane_index(shape) // nope == row_index(shape), q_nope, 0.0).astype(BF16)
    absorbed = dot(spread, w_kup_ref[...]).astype(BF16)
    turned = jnp.concatenate(
        [
            turn(q_rope[:, t * LANES : (t + 1) * LANES], cosine, sine, rope)
            for t in range(heads * rope // LANES)
        ],
        1,
    )
    shape = turned.shape
    own_lane = lane_index(shape) // rope == row_index(shape)
    spread_rope = jnp.where(own_lane, turned, 0.0).astype(BF16)
    rope_keys = jnp.concatenate([rope_ref[...]] * heads, 0)
    cached = (dot_nt(absorbed, latent_ref[...]) + dot(spread_rope, rope_keys)) * scale
    cached = jnp.where(lane_index(cached.shape) < length, cached, -1e30)
    new_latent = new_latent_ref[...].astype(F32)
    new_rope = jnp.concatenate([new_rope_ref[...].astype(F32)] * (heads * rope // LANES), 1)
    own = (
        jnp.sum(absorbed.astype(F32) * new_latent, axis=-1, keepdims=True)
        + jnp.sum(spread_rope.astype(F32) * new_rope, axis=-1, keepdims=True)
    ) * scale
    top = jnp.maximum(jnp.max(cached, axis=-1, keepdims=True), own)
    cached = jnp.exp(cached - top)
    own = jnp.exp(own - top)
    total = jnp.sum(cached, axis=-1, keepdims=True) + own
    own = (own / total).astype(BF16).astype(F32)
    context = dot((cached / total).astype(BF16), latent_ref[...]) + own * new_latent
    mixed = dot_nt(context.astype(BF16), w_vup_ref[...])
    shape = mixed.shape
    value_dim = w_vup_ref.shape[0] // heads
    mixed = jnp.where(lane_index(shape) // value_dim == row_index(shape), mixed, 0.0)
    total = jnp.sum(mixed, axis=0, keepdims=True)
    out_ref[...] = jnp.broadcast_to(total, out_ref.shape).astype(BF16)


def combine_kernel(heads, dec_ref, w_ref, *refs):
    got_refs, out_ref = refs[:-1], refs[-1]
    count = dec_ref.shape[0]
    width = w_ref.shape[0]
    value_dim = width // heads

    def read(ref):
        tail = ref[:, width:].astype(F32)
        tail = (
            tail
            + pltpu.roll(tail, LANES - heads, 1)
            + pltpu.roll(tail, LANES - 2 * heads, 1)
        )
        return tail, pltpu.roll(tail, LANES - 3 * heads, 1)

    def widen(values):
        per = LANES // value_dim
        lane = lane_index((count, LANES)) // value_dim
        tiles = []
        for t in range(width // LANES):
            tile = jnp.zeros((count, LANES), F32)
            for j in range(per):
                h = t * per + j
                tile = jnp.where(lane == j, values[:, h : h + 1], tile)
            tiles.append(tile)
        return jnp.concatenate(tiles, 1)

    stats = [read(ref) for ref in got_refs]
    best = functools.reduce(jnp.maximum, [top for top, _ in stats])
    factors = [jnp.exp(top - best) for top, _ in stats]
    total = sum(factor * total for factor, (_, total) in zip(factors, stats))
    mixed = sum(
        ref[:, :width].astype(F32) * widen(factor) for ref, factor in zip(got_refs, factors)
    )
    merged = (mixed / widen(total)).astype(BF16)
    rows = jnp.concatenate([merged, dec_ref[...]], 0)
    out_ref[...] = dot(rows, w_ref[...]).astype(BF16)


def add_kernel(*refs):
    term_refs, piece_ref, dec_ref = refs[:-2], refs[-2], refs[-1]
    total = sum(ref[...].astype(F32) for ref in term_refs)
    count = piece_ref.shape[0]
    piece_ref[...] = total[:count].astype(BF16)
    dec_ref[...] = total[count : count + 1].astype(BF16)


def call(kernel, outs, in_specs, name, flops, **extra):
    many = isinstance(outs, list)
    shapes = [jax.ShapeDtypeStruct(shape, BF16) for shape in (outs if many else [outs])]
    limit = extra.pop("limit", 8 << 20)
    specs = [VMEM] * len(shapes)
    return pl.pallas_call(
        kernel,
        out_shape=shapes if many else shapes[0],
        in_specs=in_specs,
        out_specs=specs if many else specs[0],
        name=name,
        compiler_params=pltpu.CompilerParams(vmem_limit_bytes=limit),
        cost_estimate=pl.CostEstimate(flops=flops, bytes_accessed=flops // 64, transcendentals=0),
        **extra,
    )


def shift(values, axis, step):
    size = lax.axis_size(axis)
    return lax.ppermute(values, axis, [(i, (i + step) % size) for i in range(size)])


def rope_tables(context, rows, rope):
    half = rope // 2
    inverse = ROPE_BASE ** (-np.arange(half, dtype=np.float32) * 2.0 / rope)
    inverse = inverse.astype(np.float32)
    lanes = np.tile(inverse, LANES // half)[None, :]
    angle = (context + np.arange(rows, dtype=np.float32))[:, None] * lanes
    sign = np.where(np.arange(LANES) % rope < half, -1.0, 1.0)
    return (
        np.cos(angle).astype(np.float32),
        (np.sin(angle) * sign).astype(np.float32),
        lanes.astype(np.float32),
    )


def per_device(
    piece_rows,
    decode_rows,
    prompt_latent,
    prompt_rope_key,
    decode_latent,
    decode_rope_key,
    dec_lengths,
    w_qdown,
    q_gain,
    w_qup,
    w_kvdown,
    w_krope,
    kv_gain,
    w_kup,
    w_vup,
    w_out,
):
    shards = lax.axis_size("kv")
    count, model = piece_rows.shape
    cached, width = prompt_latent.shape
    context = cached * shards
    heads, nope = w_kup.shape[1:]
    value_dim = w_vup.shape[2]
    rope = w_krope.shape[1]
    assert decode_rows.shape[0] == 1
    cosine, sine, freq = rope_tables(context, count * shards, rope)
    w_query = jnp.transpose(w_qup, (1, 2, 0))
    w_key = jnp.transpose(w_kup, (1, 2, 0)).reshape(heads * nope, width)
    w_value = jnp.transpose(w_vup, (1, 2, 0)).reshape(heads * value_dim, width)
    w_last = w_out.reshape(heads * value_dim, model)
    packed_width = heads * value_dim + LANES

    q_latent, q_decode = call(
        query_latent_kernel,
        [(count, w_qdown.shape[1]), (count, w_qdown.shape[1])],
        [VMEM, VMEM, HBM, VMEM],
        "query_latent",
        2 * 2 * count * model * w_qdown.shape[1],
        scratch_shapes=[pltpu.VMEM(w_qdown.shape, BF16), pltpu.SemaphoreType.DMA((4,))],
    )(piece_rows, decode_rows, w_qdown, q_gain[None, :])

    direct = shards <= MAX_PERMUTES
    if direct:
        steps = sorted(range(1, shards), key=lambda s: -min(s, shards - s))
        arrived = {s: shift(q_latent, "kv", s) for s in steps}
        blocks = [q_latent] + [arrived[s] for s in range(1, shards)]
    else:
        blocks = [lax.all_gather(q_latent, "kv", axis=0, tiled=True)]

    (
        piece_latent,
        dec_latent,
        piece_rope,
        dec_rope,
        keys,
        values,
        new_keys,
        new_values,
        new_rope,
        dec_latent_rows,
        dec_rope_rows,
    ) = call(
        functools.partial(keys_kernel, context),
        [
            (count, width),
            (1, width),
            (count, rope),
            (1, rope),
            (cached, heads * nope),
            (cached, heads * value_dim),
            (count, heads * nope),
            (count, heads * value_dim),
            (count, LANES),
            (count, width),
            (count, LANES),
        ],
        [SMEM] + [VMEM] * 11,
        "keys",
        4 * cached * width * heads * nope,
    )(
        dec_lengths,
        piece_rows,
        decode_rows,
        w_kvdown,
        w_krope.T,
        kv_gain[None, :],
        cosine,
        sine,
        freq,
        prompt_latent,
        w_key,
        w_value,
    )

    shared = (
        w_query,
        keys,
        values,
        new_keys,
        new_values,
        new_rope,
        prompt_rope_key.T,
        cosine,
        sine,
    )
    total_rows = count * shards
    flops = 4 * total_rows * cached * heads * nope
    if direct:
        packed = call(
            functools.partial(attend_kernel, True, nope),
            (total_rows, packed_width),
            [VMEM] * (len(shared) + shards),
            "attend",
            flops,
        )(*shared, *blocks)
        sent = [packed[s * count : (s + 1) * count] for s in range(shards)]
        came = {s: shift(sent[s], "kv", shards - s) for s in steps}
        got = [sent[0]] + [came[s] for s in range(1, shards)]
    else:
        step_rows = min(64, total_rows)
        whole = [
            pl.BlockSpec(array.shape, lambda i, rank=array.ndim: (0,) * rank) for array in shared
        ]
        packed = pl.pallas_call(
            functools.partial(attend_kernel, False, nope),
            grid=(total_rows // step_rows,),
            out_shape=jax.ShapeDtypeStruct((total_rows, packed_width), BF16),
            in_specs=whole + [pl.BlockSpec((step_rows, w_qdown.shape[1]), lambda i: (i, 0))],
            out_specs=pl.BlockSpec((step_rows, packed_width), lambda i: (i, 0)),
            name="attend",
            compiler_params=pltpu.CompilerParams(vmem_limit_bytes=24 << 20),
        )(*shared, *blocks)
        got = lax.all_to_all(packed, "kv", split_axis=0, concat_axis=0, tiled=True)
        got = [got[s * count : (s + 1) * count] for s in range(shards)]

    dec_heads = call(
        functools.partial(decode_kernel, nope),
        (count, heads * value_dim),
        [SMEM] + [VMEM] * 9,
        "decode",
        4 * count * decode_latent.shape[1] * width * 4,
    )(
        dec_lengths,
        q_decode,
        w_query,
        w_key,
        w_value,
        decode_latent[0],
        decode_rope_key[0].T,
        dec_latent_rows,
        dec_rope_rows,
        freq,
    )

    term = call(
        functools.partial(combine_kernel, heads),
        (2 * count, model),
        [VMEM] * (2 + len(got)),
        "combine",
        2 * 2 * count * heads * value_dim * model,
    )(dec_heads, w_last, *got)
    terms = [term] + [shift(term, "tp", s) for s in range(1, lax.axis_size("tp"))]
    piece_out, decode_out = call(
        add_kernel, [(count, model), (1, model)], [VMEM] * len(terms), "add", 1000
    )(*terms)
    return (piece_out, decode_out, piece_latent, piece_rope, dec_latent, dec_rope)


def solution(mesh):
    rows = P(("dp", "kv"), None)
    cube = P(("dp", "kv"), None, None)
    by_head = P(None, "tp", None)
    in_specs = (
        rows,
        rows,
        rows,
        rows,
        cube,
        cube,
        P(("dp", "kv")),
        P(),
        P(),
        by_head,
        P(),
        P(),
        P(),
        by_head,
        by_head,
        P("tp", None, None),
    )
    return jax.shard_map(
        per_device, mesh=mesh, in_specs=in_specs, out_specs=(rows,) * 6, check_vma=False
    )
```

```python
import functools

import jax
import jax.numpy as jnp
import numpy as np
from jax import lax
from jax.experimental import pallas as pl
from jax.experimental.pallas import tpu as pltpu
from jax.sharding import PartitionSpec as P

LANES = 128
GROUP = 256
MAX_PERMUTES = 8
ROPE_BASE = 10000.0
VMEM = pl.BlockSpec(memory_space=pltpu.VMEM)
SMEM = pl.BlockSpec(memory_space=pltpu.SMEM)
HBM = pl.BlockSpec(memory_space=pltpu.HBM)
NT = (((1,), (1,)), ((), ()))
F32 = jnp.float32
BF16 = jnp.bfloat16


def dot(a, b):
    return jnp.dot(a, b, preferred_element_type=F32)


def dot_nt(a, b):
    return lax.dot_general(a, b, NT, preferred_element_type=F32)


def lane_index(shape):
    return lax.broadcasted_iota(jnp.int32, shape, len(shape) - 1)


def row_index(shape):
    return lax.broadcasted_iota(jnp.int32, shape, 0)


def rms_scale(values, gain):
    return values * lax.rsqrt(jnp.mean(values * values, axis=-1, keepdims=True) + 1e-06) * gain


def turn(values, cosine, signed_sine, rope):
    half = rope // 2
    swapped = jnp.where(
        lane_index(values.shape) % rope < half,
        pltpu.roll(values, LANES - half, 1),
        pltpu.roll(values, half, 1),
    )
    return values * cosine + swapped * signed_sine


def diagonal(values, count, width):
    owner = lane_index(values.shape) // width
    return jnp.concatenate([jnp.where(owner == j, values, 0.0) for j in range(count)], 0)


def spread_rows(row, rows):
    return jnp.broadcast_to(row.astype(F32), (rows, row.shape[1])).astype(row.dtype)


def query_latent_kernel(
    piece_hbm, dec_hbm, w_hbm, gain_hbm, out_ref, dec_out_ref, piece_ref, dec_ref, gain_ref, w_ref, sems
):
    chunks = sems.shape[0] - 3
    depth = w_ref.shape[0] // chunks
    small = []
    for c, (source, target) in enumerate(
        [(piece_hbm, piece_ref), (dec_hbm, dec_ref), (gain_hbm, gain_ref)]
    ):
        small.append(pltpu.make_async_copy(source, target, sems.at[chunks + c]))
        small[-1].start()
    copies = []
    for c in range(chunks):
        part = pl.ds(c * depth, depth)
        copies.append(pltpu.make_async_copy(w_hbm.at[part], w_ref.at[part], sems.at[c]))
        copies[-1].start()
    for copy in small:
        copy.wait()
    piece = piece_ref[...]
    rows = jnp.concatenate([piece, spread_rows(dec_ref[...], piece.shape[0])], 0)
    total = jnp.zeros((rows.shape[0], w_ref.shape[1]), F32)
    for c in range(chunks):
        copies[c].wait()
        part = slice(c * depth, (c + 1) * depth)
        total = total + dot(rows[:, part], w_ref[part, :])
    latent = rms_scale(total, gain_ref[...]).astype(BF16)
    out_ref[...] = latent[: piece.shape[0]]
    dec_out_ref[...] = latent[piece.shape[0] :]


def keys_kernel(
    context,
    lengths_ref,
    piece_ref,
    dec_ref,
    w_ref,
    w_rope_ref,
    gain_ref,
    cos_ref,
    sin_ref,
    freq_ref,
    prompt_ref,
    w_kup_ref,
    w_vup_ref,
    latent_ref,
    dec_latent_ref,
    rope_ref,
    dec_rope_ref,
    key_ref,
    value_ref,
    new_key_ref,
    new_value_ref,
    new_rope_ref,
    dec_rows_ref,
    dec_rope_rows_ref,
):
    count = piece_ref.shape[0]
    rope = w_rope_ref.shape[0]
    piece = piece_ref[...]
    rows = jnp.concatenate([piece, spread_rows(dec_ref[...], count)], 0)
    latent = rms_scale(dot(rows, w_ref[...]), gain_ref[...]).astype(BF16)
    w_rope = jnp.concatenate([w_rope_ref[...]] * (LANES // rope), 0)
    raw = dot_nt(rows, w_rope)
    index = lax.axis_index("kv")
    own = pl.ds(pl.multiple_of(index * count, count), count)
    new_rope = turn(raw[:count], cos_ref[own, :], sin_ref[own, :], rope).astype(BF16)
    angle = lengths_ref[0].astype(F32) * freq_ref[...]
    sign = jnp.where(lane_index(angle.shape) % rope < rope // 2, -1.0, 1.0)
    dec_rope = turn(raw[count:], jnp.cos(angle), jnp.sin(angle) * sign, rope).astype(BF16)
    latent_ref[...] = latent[:count]
    dec_latent_ref[...] = latent[count : count + 1]
    rope_ref[...] = new_rope[:, :rope]
    dec_rope_ref[...] = dec_rope[:1, :rope]
    new_rope_ref[...] = new_rope
    dec_rows_ref[...] = latent[count:]
    dec_rope_rows_ref[...] = dec_rope
    w_kup, w_vup = w_kup_ref[...], w_vup_ref[...]
    prompt = prompt_ref[...]
    key_ref[...] = dot_nt(prompt, w_kup).astype(BF16)
    value_ref[...] = dot_nt(prompt, w_vup).astype(BF16)
    new_key_ref[...] = dot_nt(latent[:count], w_kup).astype(BF16)
    new_value_ref[...] = dot_nt(latent[:count], w_vup).astype(BF16)


def split_query_weights(w_ref, nope):
    heads = w_ref.shape[0]
    w_nope = jnp.concatenate([w_ref[h, :nope, :] for h in range(heads)], 0)
    w_rope = jnp.concatenate([w_ref[h, nope:, :] for h in range(heads)], 0)
    return w_nope, w_rope


def attend_kernel(relative, nope, *refs):
    (
        w_ref,
        key_ref,
        value_ref,
        new_key_ref,
        new_value_ref,
        new_rope_ref,
        rope_ref,
        cos_ref,
        sin_ref,
    ) = refs[:9]
    latent_refs, out_ref = refs[9:-1], refs[-1]
    shards = lax.axis_size("kv")
    index = lax.axis_index("kv")
    heads = w_ref.shape[0]
    rope = w_ref.shape[1] - nope
    count = new_key_ref.shape[0]
    latents = jnp.concatenate([ref[...] for ref in latent_refs], 0)
    queries = latents.shape[0]
    blocks = queries // count
    first = 0 if relative else pl.program_id(0) * blocks
    owners = []
    for s in range(blocks):
        owners.append(lax.rem(index - s + shards, shards) if relative else first + s)
    tables = [pl.ds(pl.multiple_of(owner * count, count), count) for owner in owners]
    cosine = jnp.concatenate([cos_ref[part, :] for part in tables], 0)
    sine = jnp.concatenate([sin_ref[part, :] for part in tables], 0)
    scale = (nope + rope) ** (-0.5)
    w_nope, w_rope = split_query_weights(w_ref, nope)
    q_nope = dot_nt(latents, w_nope).astype(BF16).astype(F32)
    q_rope = dot_nt(latents, w_rope)
    per = GROUP // nope
    rope_keys = jnp.concatenate([rope_ref[...]] * (LANES // rope), 0)
    new_rope = new_rope_ref[...]
    row = row_index((count, count))
    column = lane_index((count, count))
    allowed = jnp.concatenate(
        [index * count + column <= owner * count + row for owner in owners] * per, 0
    )
    lane = lane_index((queries, LANES))
    stats = jnp.zeros((queries, LANES), F32)
    for g in range(heads // per):
        wide = slice(g * GROUP, (g + 1) * GROUP)
        turned = turn(q_rope[:, g * LANES : (g + 1) * LANES], cosine, sine, rope)
        spread = diagonal(q_nope[:, wide], per, nope).astype(BF16)
        spread_rope = diagonal(turned, per, rope).astype(BF16)
        old = (dot_nt(spread, key_ref[:, wide]) + dot(spread_rope, rope_keys)) * scale
        new = (dot_nt(spread, new_key_ref[:, wide]) + dot_nt(spread_rope, new_rope)) * scale
        new = jnp.where(allowed, new, -1e30)
        top = jnp.maximum(
            jnp.max(old, axis=-1, keepdims=True), jnp.max(new, axis=-1, keepdims=True)
        )
        old = jnp.exp(old - top)
        new = jnp.exp(new - top)
        total = jnp.sum(old, axis=-1, keepdims=True) + jnp.sum(new, axis=-1, keepdims=True)
        mixed = dot(old.astype(BF16), value_ref[:, wide]) + dot(
            new.astype(BF16), new_value_ref[:, wide]
        )
        owner_lane = lane_index((queries, GROUP)) // nope
        part = jnp.zeros((queries, GROUP), F32)
        for j in range(per):
            own = slice(j * queries, (j + 1) * queries)
            part = jnp.where(owner_lane == j, mixed[own], part)
            h = g * per + j
            stats = jnp.where(
                lane % heads == h, jnp.where(lane < 3 * heads, top[own], total[own]), stats
            )
        out_ref[:, wide] = part.astype(BF16)
    high = stats.astype(BF16).astype(F32)
    rest = stats - high
    middle = rest.astype(BF16).astype(F32)
    piece = (lane // heads) % 3
    stats = jnp.where(piece == 0, high, jnp.where(piece == 1, middle, rest - middle))
    stats = jnp.where(lane < 6 * heads, stats, 0.0)
    out_ref[:, heads * nope :] = stats.astype(BF16)


def decode_kernel(
    nope,
    lengths_ref,
    q_ref,
    w_ref,
    w_kup_ref,
    w_vup_ref,
    latent_ref,
    rope_ref,
    new_latent_ref,
    new_rope_ref,
    freq_ref,
    out_ref,
):
    heads = w_ref.shape[0]
    rope = w_ref.shape[1] - nope
    length = lengths_ref[0]
    scale = (nope + rope) ** (-0.5)
    latents = q_ref[...]
    rows = latents.shape[0]
    w_nope, w_rope = split_query_weights(w_ref, nope)
    q_nope = dot_nt(latents, w_nope)
    q_rope = dot_nt(latents, w_rope)
    angle = length.astype(F32) * freq_ref[...]
    sign = jnp.where(lane_index(angle.shape) % rope < rope // 2, -1.0, 1.0)
    cosine, sine = jnp.cos(angle), jnp.sin(angle) * sign
    shape = q_nope.shape
    spread = jnp.where(lane_index(shape) // nope == row_index(shape), q_nope, 0.0).astype(BF16)
    absorbed = dot(spread, w_kup_ref[...]).astype(BF16)
    turned = jnp.concatenate(
        [
            turn(q_rope[:, t * LANES : (t + 1) * LANES], cosine, sine, rope)
            for t in range(heads * rope // LANES)
        ],
        1,
    )
    shape = turned.shape
    own_lane = lane_index(shape) // rope == row_index(shape)
    spread_rope = jnp.where(own_lane, turned, 0.0).astype(BF16)
    rope_keys = jnp.concatenate([rope_ref[...]] * heads, 0)
    cached = (dot_nt(absorbed, latent_ref[...]) + dot(spread_rope, rope_keys)) * scale
    cached = jnp.where(lane_index(cached.shape) < length, cached, -1e30)
    new_latent = new_latent_ref[...].astype(F32)
    new_rope = jnp.concatenate([new_rope_ref[...].astype(F32)] * (heads * rope // LANES), 1)
    own = (
        jnp.sum(absorbed.astype(F32) * new_latent, axis=-1, keepdims=True)
        + jnp.sum(spread_rope.astype(F32) * new_rope, axis=-1, keepdims=True)
    ) * scale
    top = jnp.maximum(jnp.max(cached, axis=-1, keepdims=True), own)
    cached = jnp.exp(cached - top)
    own = jnp.exp(own - top)
    total = jnp.sum(cached, axis=-1, keepdims=True) + own
    own = (own / total).astype(BF16).astype(F32)
    context = dot((cached / total).astype(BF16), latent_ref[...]) + own * new_latent
    mixed = dot_nt(context.astype(BF16), w_vup_ref[...])
    shape = mixed.shape
    value_dim = w_vup_ref.shape[0] // heads
    mixed = jnp.where(lane_index(shape) // value_dim == row_index(shape), mixed, 0.0)
    total = jnp.sum(mixed, axis=0, keepdims=True)
    out_ref[...] = jnp.broadcast_to(total, out_ref.shape).astype(BF16)


def combine_kernel(heads, dec_ref, w_ref, *refs):
    got_refs, out_ref = refs[:-1], refs[-1]
    count = dec_ref.shape[0]
    width = w_ref.shape[0]
    value_dim = width // heads

    def read(ref):
        tail = ref[:, width:].astype(F32)
        tail = (
            tail
            + pltpu.roll(tail, LANES - heads, 1)
            + pltpu.roll(tail, LANES - 2 * heads, 1)
        )
        return tail, pltpu.roll(tail, LANES - 3 * heads, 1)

    def widen(values):
        per = LANES // value_dim
        lane = lane_index((count, LANES)) // value_dim
        tiles = []
        for t in range(width // LANES):
            tile = jnp.zeros((count, LANES), F32)
            for j in range(per):
                h = t * per + j
                tile = jnp.where(lane == j, values[:, h : h + 1], tile)
            tiles.append(tile)
        return jnp.concatenate(tiles, 1)

    stats = [read(ref) for ref in got_refs]
    best = functools.reduce(jnp.maximum, [top for top, _ in stats])
    factors = [jnp.exp(top - best) for top, _ in stats]
    total = sum(factor * total for factor, (_, total) in zip(factors, stats))
    mixed = sum(
        ref[:, :width].astype(F32) * widen(factor) for ref, factor in zip(got_refs, factors)
    )
    merged = (mixed / widen(total)).astype(BF16)
    rows = jnp.concatenate([merged, dec_ref[...]], 0)
    out_ref[...] = dot(rows, w_ref[...]).astype(BF16)


def add_kernel(*refs):
    term_refs, piece_ref, dec_ref = refs[:-2], refs[-2], refs[-1]
    total = sum(ref[...].astype(F32) for ref in term_refs)
    count = piece_ref.shape[0]
    piece_ref[...] = total[:count].astype(BF16)
    dec_ref[...] = total[count : count + 1].astype(BF16)


def call(kernel, outs, in_specs, name, flops, **extra):
    many = isinstance(outs, list)
    shapes = [jax.ShapeDtypeStruct(shape, BF16) for shape in (outs if many else [outs])]
    limit = extra.pop("limit", 8 << 20)
    specs = [VMEM] * len(shapes)
    return pl.pallas_call(
        kernel,
        out_shape=shapes if many else shapes[0],
        in_specs=in_specs,
        out_specs=specs if many else specs[0],
        name=name,
        compiler_params=pltpu.CompilerParams(vmem_limit_bytes=limit),
        cost_estimate=pl.CostEstimate(flops=flops, bytes_accessed=flops // 64, transcendentals=0),
        **extra,
    )


def shift(values, axis, step):
    size = lax.axis_size(axis)
    return lax.ppermute(values, axis, [(i, (i + step) % size) for i in range(size)])


def in_hbm(array):
    return pltpu.with_memory_space_constraint(array, pltpu.HBM)


def rope_tables(context, rows, rope):
    half = rope // 2
    inverse = ROPE_BASE ** (-np.arange(half, dtype=np.float32) * 2.0 / rope)
    inverse = inverse.astype(np.float32)
    lanes = np.tile(inverse, LANES // half)[None, :]
    angle = (context + np.arange(rows, dtype=np.float32))[:, None] * lanes
    sign = np.where(np.arange(LANES) % rope < half, -1.0, 1.0)
    return (
        np.cos(angle).astype(np.float32),
        (np.sin(angle) * sign).astype(np.float32),
        lanes.astype(np.float32),
    )


def per_device(
    piece_rows,
    decode_rows,
    prompt_latent,
    prompt_rope_key,
    decode_latent,
    decode_rope_key,
    dec_lengths,
    w_qdown,
    q_gain,
    w_qup,
    w_kvdown,
    w_krope,
    kv_gain,
    w_kup,
    w_vup,
    w_out,
):
    shards = lax.axis_size("kv")
    count, model = piece_rows.shape
    cached, width = prompt_latent.shape
    context = cached * shards
    heads, nope = w_kup.shape[1:]
    value_dim = w_vup.shape[2]
    rope = w_krope.shape[1]
    assert decode_rows.shape[0] == 1
    cosine, sine, freq = rope_tables(context, count * shards, rope)
    w_query = jnp.transpose(w_qup, (1, 2, 0))
    w_key = jnp.transpose(w_kup, (1, 2, 0)).reshape(heads * nope, width)
    w_value = jnp.transpose(w_vup, (1, 2, 0)).reshape(heads * value_dim, width)
    w_last = w_out.reshape(heads * value_dim, model)
    packed_width = heads * value_dim + LANES

    q_latent, q_decode = call(
        query_latent_kernel,
        [(count, w_qdown.shape[1]), (count, w_qdown.shape[1])],
        [HBM, HBM, HBM, HBM],
        "query_latent",
        2 * 2 * count * model * w_qdown.shape[1] * 100,
        scratch_shapes=[
            pltpu.VMEM(piece_rows.shape, BF16),
            pltpu.VMEM(decode_rows.shape, BF16),
            pltpu.VMEM((1, q_gain.shape[0]), F32),
            pltpu.VMEM(w_qdown.shape, BF16),
            pltpu.SemaphoreType.DMA((7,)),
        ],
    )(*[in_hbm(array) for array in (piece_rows, decode_rows, w_qdown, q_gain[None, :])])

    direct = shards <= MAX_PERMUTES
    if direct:
        steps = sorted(range(1, shards), key=lambda s: -min(s, shards - s))
        arrived = {s: shift(q_latent, "kv", s) for s in steps}
        blocks = [q_latent] + [arrived[s] for s in range(1, shards)]
    else:
        blocks = [lax.all_gather(q_latent, "kv", axis=0, tiled=True)]

    (
        piece_latent,
        dec_latent,
        piece_rope,
        dec_rope,
        keys,
        values,
        new_keys,
        new_values,
        new_rope,
        dec_latent_rows,
        dec_rope_rows,
    ) = call(
        functools.partial(keys_kernel, context),
        [
            (count, width),
            (1, width),
            (count, rope),
            (1, rope),
            (cached, heads * nope),
            (cached, heads * value_dim),
            (count, heads * nope),
            (count, heads * value_dim),
            (count, LANES),
            (count, width),
            (count, LANES),
        ],
        [SMEM] + [VMEM] * 11,
        "keys",
        4 * cached * width * heads * nope,
    )(
        dec_lengths,
        piece_rows,
        decode_rows,
        w_kvdown,
        w_krope.T,
        kv_gain[None, :],
        cosine,
        sine,
        freq,
        prompt_latent,
        w_key,
        w_value,
    )

    shared = (
        w_query,
        keys,
        values,
        new_keys,
        new_values,
        new_rope,
        prompt_rope_key.T,
        cosine,
        sine,
    )
    total_rows = count * shards
    flops = 4 * total_rows * cached * heads * nope
    if direct:
        packed = call(
            functools.partial(attend_kernel, True, nope),
            (total_rows, packed_width),
            [VMEM] * (len(shared) + shards),
            "attend",
            flops,
        )(*shared, *blocks)
        sent = [packed[s * count : (s + 1) * count] for s in range(shards)]
        came = {s: shift(sent[s], "kv", shards - s) for s in steps}
        got = [sent[0]] + [came[s] for s in range(1, shards)]
    else:
        step_rows = min(64, total_rows)
        whole = [
            pl.BlockSpec(array.shape, lambda i, rank=array.ndim: (0,) * rank) for array in shared
        ]
        packed = pl.pallas_call(
            functools.partial(attend_kernel, False, nope),
            grid=(total_rows // step_rows,),
            out_shape=jax.ShapeDtypeStruct((total_rows, packed_width), BF16),
            in_specs=whole + [pl.BlockSpec((step_rows, w_qdown.shape[1]), lambda i: (i, 0))],
            out_specs=pl.BlockSpec((step_rows, packed_width), lambda i: (i, 0)),
            name="attend",
            compiler_params=pltpu.CompilerParams(vmem_limit_bytes=24 << 20),
        )(*shared, *blocks)
        got = lax.all_to_all(packed, "kv", split_axis=0, concat_axis=0, tiled=True)
        got = [got[s * count : (s + 1) * count] for s in range(shards)]

    dec_heads = call(
        functools.partial(decode_kernel, nope),
        (count, heads * value_dim),
        [SMEM] + [VMEM] * 9,
        "decode",
        4 * count * decode_latent.shape[1] * width * 4,
    )(
        dec_lengths,
        q_decode,
        w_query,
        w_key,
        w_value,
        decode_latent[0],
        decode_rope_key[0].T,
        dec_latent_rows,
        dec_rope_rows,
        freq,
    )

    term = call(
        functools.partial(combine_kernel, heads),
        (2 * count, model),
        [VMEM] * (2 + len(got)),
        "combine",
        2 * 2 * count * heads * value_dim * model,
    )(dec_heads, w_last, *got)
    terms = [term] + [shift(term, "tp", s) for s in range(1, lax.axis_size("tp"))]
    piece_out, decode_out = call(
        add_kernel, [(count, model), (1, model)], [VMEM] * len(terms), "add", 1000
    )(*terms)
    return (piece_out, decode_out, piece_latent, piece_rope, dec_latent, dec_rope)


def solution(mesh):
    rows = P(("dp", "kv"), None)
    cube = P(("dp", "kv"), None, None)
    by_head = P(None, "tp", None)
    in_specs = (
        rows,
        rows,
        rows,
        rows,
        cube,
        cube,
        P(("dp", "kv")),
        P(),
        P(),
        by_head,
        P(),
        P(),
        P(),
        by_head,
        by_head,
        P("tp", None, None),
    )
    return jax.shard_map(
        per_device, mesh=mesh, in_specs=in_specs, out_specs=(rows,) * 6, check_vma=False
    )
```

```python
import functools

import jax
import jax.numpy as jnp
import numpy as np
from jax import lax
from jax.experimental import pallas as pl
from jax.experimental.pallas import tpu as pltpu
from jax.sharding import PartitionSpec as P

LANES = 128
GROUP = 256
MAX_PERMUTES = 8
ROPE_BASE = 10000.0
VMEM = pl.BlockSpec(memory_space=pltpu.VMEM)
HBM = pl.BlockSpec(memory_space=pltpu.HBM)
NT = (((1,), (1,)), ((), ()))
F32 = jnp.float32
BF16 = jnp.bfloat16


def dot(a, b):
    return jnp.dot(a, b, preferred_element_type=F32)


def dot_nt(a, b):
    return lax.dot_general(a, b, NT, preferred_element_type=F32)


def lane_index(shape):
    return lax.broadcasted_iota(jnp.int32, shape, len(shape) - 1)


def row_index(shape):
    return lax.broadcasted_iota(jnp.int32, shape, 0)


def rms_scale(values, gain):
    return values * lax.rsqrt(jnp.mean(values * values, axis=-1, keepdims=True) + 1e-06) * gain


def turn(values, cosine, signed_sine, rope):
    half = rope // 2
    swapped = jnp.where(
        lane_index(values.shape) % rope < half,
        pltpu.roll(values, LANES - half, 1),
        pltpu.roll(values, half, 1),
    )
    return values * cosine + swapped * signed_sine


def diagonal(values, count, width):
    owner = lane_index(values.shape) // width
    return jnp.concatenate([jnp.where(owner == j, values, 0.0) for j in range(count)], 0)


def spread_rows(row, rows):
    return jnp.broadcast_to(row.astype(F32), (rows, row.shape[1])).astype(row.dtype)


def query_latent_kernel(
    piece_hbm,
    dec_hbm,
    w_hbm,
    gain_hbm,
    out_ref,
    dec_out_ref,
    piece_ref,
    dec_ref,
    gain_ref,
    w_ref,
    sems,
):
    chunks = sems.shape[0] - 3
    depth = w_ref.shape[0] // chunks
    small = []
    for c, (source, target) in enumerate(
        [
            (piece_hbm, piece_ref),
            (dec_hbm, dec_ref),
            (gain_hbm, gain_ref),
        ]
    ):
        small.append(pltpu.make_async_copy(source, target, sems.at[chunks + c]))
        small[-1].start()
    copies = []
    for c in range(chunks):
        part = pl.ds(c * depth, depth)
        copies.append(pltpu.make_async_copy(w_hbm.at[part], w_ref.at[part], sems.at[c]))
        copies[-1].start()
    for copy in small:
        copy.wait()
    piece = piece_ref[...]
    rows = jnp.concatenate([piece, spread_rows(dec_ref[...], piece.shape[0])], 0)
    total = jnp.zeros((rows.shape[0], w_ref.shape[1]), F32)
    for c in range(chunks):
        copies[c].wait()
        part = slice(c * depth, (c + 1) * depth)
        total = total + dot(rows[:, part], w_ref[part, :])
    latent = rms_scale(total, gain_ref[...]).astype(BF16)
    out_ref[...] = latent[: piece.shape[0]]
    dec_out_ref[...] = latent[piece.shape[0] :]


def keys_kernel(
    context,
    lengths_ref,
    piece_ref,
    dec_ref,
    w_ref,
    w_rope_ref,
    gain_ref,
    cos_ref,
    sin_ref,
    freq_ref,
    prompt_ref,
    w_kup_ref,
    w_vup_ref,
    latent_ref,
    dec_latent_ref,
    rope_ref,
    dec_rope_ref,
    key_ref,
    value_ref,
    new_key_ref,
    new_value_ref,
):
    count = piece_ref.shape[0]
    rope = w_rope_ref.shape[0]
    piece = piece_ref[...]
    rows = jnp.concatenate([piece, spread_rows(dec_ref[...], count)], 0)
    latent = rms_scale(dot(rows, w_ref[...]), gain_ref[...]).astype(BF16)
    w_rope = jnp.concatenate([w_rope_ref[...]] * (LANES // rope), 0)
    raw = dot_nt(rows, w_rope)
    index = lax.axis_index("kv")
    own = pl.ds(pl.multiple_of(index * count, count), count)
    new_rope = turn(raw[:count], cos_ref[own, :], sin_ref[own, :], rope).astype(BF16)
    angle = lengths_ref[...] * freq_ref[...]
    sign = jnp.where(lane_index(angle.shape) % rope < rope // 2, -1.0, 1.0)
    dec_rope = turn(raw[count:], jnp.cos(angle), jnp.sin(angle) * sign, rope).astype(BF16)
    latent_ref[...] = latent[:count]
    dec_latent_ref[...] = latent[count:]
    rope_ref[...] = new_rope
    dec_rope_ref[...] = dec_rope
    w_kup, w_vup = w_kup_ref[...], w_vup_ref[...]
    prompt = prompt_ref[...]
    key_ref[...] = dot_nt(prompt, w_kup).astype(BF16)
    value_ref[...] = dot_nt(prompt, w_vup).astype(BF16)
    new_key_ref[...] = dot_nt(latent[:count], w_kup).astype(BF16)
    new_value_ref[...] = dot_nt(latent[:count], w_vup).astype(BF16)


def split_query_weights(w_ref, nope):
    heads = w_ref.shape[0]
    w_nope = jnp.concatenate([w_ref[h, :nope, :] for h in range(heads)], 0)
    w_rope = jnp.concatenate([w_ref[h, nope:, :] for h in range(heads)], 0)
    return w_nope, w_rope


def attend_kernel(slots, nope, *refs):
    (
        w_ref,
        key_ref,
        value_ref,
        new_key_ref,
        new_value_ref,
        new_rope_ref,
        rope_ref,
        cos_ref,
        sin_ref,
    ) = refs[:9]
    index = lax.axis_index("kv")
    part = lax.axis_index("tp")
    if slots:
        shards = len(slots)
        latent_refs, out_refs, out_ref = refs[9 : 9 + shards], refs[9 + shards : -1], refs[-1]
    else:
        latent_refs, out_ref = refs[9:-1], refs[-1]
    heads = w_ref.shape[0]
    rope = w_ref.shape[1] - nope
    count = new_key_ref.shape[0]
    latents = jnp.concatenate([ref[...] for ref in latent_refs], 0)
    if slots:
        owners = [lax.rem(index - pick(part, steps) + shards, shards) for steps in slots]
    else:
        first = pl.program_id(0) * (latents.shape[0] // count)
        owners = [first + s for s in range(latents.shape[0] // count)]
    queries = latents.shape[0]
    tables = [pl.ds(pl.multiple_of(owner * count, count), count) for owner in owners]
    cosine = jnp.concatenate([cos_ref[part, :] for part in tables], 0)
    sine = jnp.concatenate([sin_ref[part, :] for part in tables], 0)
    scale = (nope + rope) ** (-0.5)
    w_nope, w_rope = split_query_weights(w_ref, nope)
    q_nope = dot_nt(latents, w_nope).astype(BF16).astype(F32)
    q_rope = dot_nt(latents, w_rope)
    per = GROUP // nope
    rope_keys = jnp.concatenate([rope_ref[...]] * (LANES // rope), 0)
    new_rope = new_rope_ref[...]
    row = row_index((count, count))
    column = lane_index((count, count))
    allowed = jnp.concatenate(
        [index * count + column <= owner * count + row for owner in owners] * per, 0
    )
    lane = lane_index((queries, LANES))
    stats = jnp.zeros((queries, LANES), F32)
    for g in range(heads // per):
        wide = slice(g * GROUP, (g + 1) * GROUP)
        turned = turn(q_rope[:, g * LANES : (g + 1) * LANES], cosine, sine, rope)
        spread = diagonal(q_nope[:, wide], per, nope).astype(BF16)
        spread_rope = diagonal(turned, per, rope).astype(BF16)
        old = (dot_nt(spread, key_ref[:, wide]) + dot(spread_rope, rope_keys)) * scale
        new = (dot_nt(spread, new_key_ref[:, wide]) + dot_nt(spread_rope, new_rope)) * scale
        new = jnp.where(allowed, new, -1e30)
        top = jnp.maximum(
            jnp.max(old, axis=-1, keepdims=True), jnp.max(new, axis=-1, keepdims=True)
        )
        old = jnp.exp(old - top)
        new = jnp.exp(new - top)
        total = jnp.sum(old, axis=-1, keepdims=True) + jnp.sum(new, axis=-1, keepdims=True)
        mixed = dot(old.astype(BF16), value_ref[:, wide]) + dot(
            new.astype(BF16), new_value_ref[:, wide]
        )
        owner_lane = lane_index((queries, GROUP)) // nope
        kept = jnp.zeros((queries, GROUP), F32)
        for j in range(per):
            own = slice(j * queries, (j + 1) * queries)
            kept = jnp.where(owner_lane == j, mixed[own], kept)
            h = g * per + j
            stats = jnp.where(
                lane % heads == h, jnp.where(lane < 3 * heads, top[own], total[own]), stats
            )
        out_ref[:, wide] = kept.astype(BF16)
    high = stats.astype(BF16).astype(F32)
    rest = stats - high
    middle = rest.astype(BF16).astype(F32)
    piece = (lane // heads) % 3
    stats = jnp.where(piece == 0, high, jnp.where(piece == 1, middle, rest - middle))
    stats = jnp.where(lane < 6 * heads, stats, 0.0)
    out_ref[:, heads * nope :] = stats.astype(BF16)
    if slots:
        for back, ref in enumerate(out_refs):
            places = [[steps[t] for steps in slots].index(back) for t in range(len(slots[0]))]
            ref[...] = block_at(out_ref, pick(part, places), count)


def decode_kernel(
    nope,
    lengths_ref,
    q_ref,
    w_ref,
    w_kup_ref,
    w_vup_ref,
    latent_ref,
    rope_ref,
    new_latent_ref,
    new_rope_ref,
    freq_ref,
    piece_latent_ref,
    piece_rope_ref,
    out_ref,
    latent_out_ref,
    dec_latent_out_ref,
    rope_out_ref,
    dec_rope_out_ref,
):
    heads = w_ref.shape[0]
    rope = w_ref.shape[1] - nope
    latent_out_ref[...] = piece_latent_ref[...]
    dec_latent_out_ref[...] = new_latent_ref[:1, :]
    rope_out_ref[...] = piece_rope_ref[:, :rope]
    dec_rope_out_ref[...] = new_rope_ref[:1, :rope]
    length = lengths_ref[...]
    scale = (nope + rope) ** (-0.5)
    latents = q_ref[...]
    rows = latents.shape[0]
    w_nope, w_rope = split_query_weights(w_ref, nope)
    q_nope = dot_nt(latents, w_nope)
    q_rope = dot_nt(latents, w_rope)
    angle = length * freq_ref[...]
    sign = jnp.where(lane_index(angle.shape) % rope < rope // 2, -1.0, 1.0)
    cosine, sine = jnp.cos(angle), jnp.sin(angle) * sign
    shape = q_nope.shape
    spread = jnp.where(lane_index(shape) // nope == row_index(shape), q_nope, 0.0).astype(BF16)
    absorbed = dot(spread, w_kup_ref[...]).astype(BF16)
    turned = jnp.concatenate(
        [
            turn(q_rope[:, t * LANES : (t + 1) * LANES], cosine, sine, rope)
            for t in range(heads * rope // LANES)
        ],
        1,
    )
    shape = turned.shape
    own_lane = lane_index(shape) // rope == row_index(shape)
    spread_rope = jnp.where(own_lane, turned, 0.0).astype(BF16)
    rope_keys = jnp.concatenate([rope_ref[...]] * heads, 0)
    cached = (dot_nt(absorbed, latent_ref[...]) + dot(spread_rope, rope_keys)) * scale
    cached = jnp.where(lane_index(cached.shape).astype(F32) < length[:, :1], cached, -1e30)
    new_latent = new_latent_ref[...].astype(F32)
    new_rope = jnp.concatenate([new_rope_ref[...].astype(F32)] * (heads * rope // LANES), 1)
    own = (
        jnp.sum(absorbed.astype(F32) * new_latent, axis=-1, keepdims=True)
        + jnp.sum(spread_rope.astype(F32) * new_rope, axis=-1, keepdims=True)
    ) * scale
    top = jnp.maximum(jnp.max(cached, axis=-1, keepdims=True), own)
    cached = jnp.exp(cached - top)
    own = jnp.exp(own - top)
    total = jnp.sum(cached, axis=-1, keepdims=True) + own
    own = (own / total).astype(BF16).astype(F32)
    context = dot((cached / total).astype(BF16), latent_ref[...]) + own * new_latent
    mixed = dot_nt(context.astype(BF16), w_vup_ref[...])
    shape = mixed.shape
    value_dim = w_vup_ref.shape[0] // heads
    mixed = jnp.where(lane_index(shape) // value_dim == row_index(shape), mixed, 0.0)
    total = jnp.sum(mixed, axis=0, keepdims=True)
    out_ref[...] = jnp.broadcast_to(total, out_ref.shape).astype(BF16)


def combine_kernel(heads, dec_ref, w_ref, *refs):
    count = dec_ref.shape[0]
    got, out_ref = [ref[...] for ref in refs[:-1]], refs[-1]
    width = w_ref.shape[0]
    value_dim = width // heads

    def read(block):
        tail = block[:, width:].astype(F32)
        tail = (
            tail
            + pltpu.roll(tail, LANES - heads, 1)
            + pltpu.roll(tail, LANES - 2 * heads, 1)
        )
        return tail, pltpu.roll(tail, LANES - 3 * heads, 1)

    def widen(values):
        per = LANES // value_dim
        lane = lane_index((count, LANES)) // value_dim
        tiles = []
        for t in range(width // LANES):
            tile = jnp.zeros((count, LANES), F32)
            for j in range(per):
                h = t * per + j
                tile = jnp.where(lane == j, values[:, h : h + 1], tile)
            tiles.append(tile)
        return jnp.concatenate(tiles, 1)

    stats = [read(block) for block in got]
    best = functools.reduce(jnp.maximum, [top for top, _ in stats])
    factors = [jnp.exp(top - best) for top, _ in stats]
    total = sum(factor * total for factor, (_, total) in zip(factors, stats))
    mixed = sum(
        block[:, :width].astype(F32) * widen(factor) for block, factor in zip(got, factors)
    )
    merged = (mixed / widen(total)).astype(BF16)
    rows = jnp.concatenate([merged, dec_ref[...]], 0)
    out_ref[...] = dot(rows, w_ref[...]).astype(BF16)


def add_kernel(*refs):
    term_refs, piece_ref, dec_ref = refs[:-2], refs[-2], refs[-1]
    total = sum(ref[...].astype(F32) for ref in term_refs)
    count = piece_ref.shape[0]
    piece_ref[...] = total[:count].astype(BF16)
    dec_ref[...] = total[count : count + 1].astype(BF16)


def call(kernel, outs, in_specs, name, flops, **extra):
    many = isinstance(outs, list)
    shapes = []
    for out in outs if many else [outs]:
        shapes.append(jax.ShapeDtypeStruct(out, BF16))
    limit = extra.pop("limit", 8 << 20)
    specs = [VMEM] * len(shapes)
    return pl.pallas_call(
        kernel,
        out_shape=shapes if many else shapes[0],
        in_specs=in_specs,
        out_specs=specs if many else specs[0],
        name=name,
        compiler_params=pltpu.CompilerParams(vmem_limit_bytes=limit),
        cost_estimate=pl.CostEstimate(flops=flops, bytes_accessed=flops // 64, transcendentals=0),
        **extra,
    )


def ring_pairs(shards, step):
    return [(i, (i + step) % shards) for i in range(shards)]


def mixed_pairs(shards, parts, taken):
    return [
        (i * parts + t, (i + taken[t % len(taken)]) % shards * parts + t)
        for i in range(shards)
        for t in range(parts)
    ]


def swap(values, axis, step):
    return lax.ppermute(values, axis, ring_pairs(lax.axis_size(axis), step))


def gather_plan(shards, parts):
    steps = list(range(1, shards))
    plan = []
    while steps:
        together = parts if parts == 2 and len(steps) >= 2 else 1
        plan.append(steps[:together])
        steps = steps[together:]
    return plan


def slot_steps(plan, parts):
    slots = [[0] * parts]
    for taken in plan:
        for turned in range(len(taken)):
            slots.append([taken[(t + turned) % len(taken)] for t in range(parts)])
    return slots


def pick(index, values):
    chosen = jnp.int32(values[0])
    for i, value in enumerate(values):
        if value != values[0]:
            chosen = jnp.where(index == i, value, chosen)
    return chosen


def block_at(ref, number, count):
    return ref[pl.ds(pl.multiple_of(number * count, count), count), :]


def in_hbm(array):
    return pltpu.with_memory_space_constraint(array, pltpu.HBM)


def rope_tables(context, rows, rope):
    half = rope // 2
    inverse = ROPE_BASE ** (-np.arange(half, dtype=np.float32) * 2.0 / rope)
    inverse = inverse.astype(np.float32)
    lanes = np.tile(inverse, LANES // half)[None, :]
    angle = (context + np.arange(rows, dtype=np.float32))[:, None] * lanes
    sign = np.where(np.arange(LANES) % rope < half, -1.0, 1.0)
    return (
        np.cos(angle).astype(np.float32),
        (np.sin(angle) * sign).astype(np.float32),
        lanes.astype(np.float32),
    )


def per_device(
    piece_rows,
    decode_rows,
    prompt_latent,
    prompt_rope_key,
    decode_latent,
    decode_rope_key,
    dec_lengths,
    w_qdown,
    q_gain,
    w_qup,
    w_kvdown,
    w_krope,
    kv_gain,
    w_kup,
    w_vup,
    w_out,
):
    shards, parts = lax.axis_size("kv"), lax.axis_size("tp")
    count, model = piece_rows.shape
    cached, width = prompt_latent.shape
    context = cached * shards
    heads, nope = w_kup.shape[1:]
    value_dim = w_vup.shape[2]
    rope = w_krope.shape[1]
    assert decode_rows.shape[0] == 1
    cosine, sine, freq = rope_tables(context, count * shards, rope)
    w_query = jnp.transpose(w_qup, (1, 2, 0))
    w_key = jnp.transpose(w_kup, (1, 2, 0)).reshape(heads * nope, width)
    w_value = jnp.transpose(w_vup, (1, 2, 0)).reshape(heads * value_dim, width)
    w_last = w_out.reshape(heads * value_dim, model)
    packed_width = heads * value_dim + LANES

    q_latent, q_decode = call(
        query_latent_kernel,
        [(count, w_qdown.shape[1]), (count, w_qdown.shape[1])],
        [HBM] * 4,
        "query_latent",
        2 * 2 * count * model * w_qdown.shape[1] * 100,
        scratch_shapes=[
            pltpu.VMEM(piece_rows.shape, BF16),
            pltpu.VMEM(decode_rows.shape, BF16),
            pltpu.VMEM((1, q_gain.shape[0]), F32),
            pltpu.VMEM(w_qdown.shape, BF16),
            pltpu.SemaphoreType.DMA((4 + 3,)),
        ],
    )(*[in_hbm(array) for array in (piece_rows, decode_rows, w_qdown, q_gain[None, :])])

    length = jnp.broadcast_to(dec_lengths.astype(F32)[:, None], (1, LANES))
    direct = shards <= MAX_PERMUTES
    if direct:
        plan = gather_plan(shards, parts)
        slots = slot_steps(plan, parts)
        blocks = [q_latent]
        for taken in plan:
            blocks.append(lax.ppermute(q_latent, ("kv", "tp"), mixed_pairs(shards, parts, taken)))
            if len(taken) > 1:
                blocks.append(swap(blocks[-1], "tp", 1))
    else:
        blocks = [lax.all_gather(q_latent, "kv", axis=0, tiled=True)]

    new_latent, dec_latent_rows, new_rope, dec_rope_rows, keys, values, new_keys, new_values = call(
        functools.partial(keys_kernel, context),
        [
            (count, width),
            (count, width),
            (count, LANES),
            (count, LANES),
            (cached, heads * nope),
            (cached, heads * value_dim),
            (count, heads * nope),
            (count, heads * value_dim),
        ],
        [VMEM] * 12,
        "keys",
        4 * cached * width * heads * nope,
    )(
        length,
        piece_rows,
        decode_rows,
        w_kvdown,
        w_krope.T,
        kv_gain[None, :],
        cosine,
        sine,
        freq,
        prompt_latent,
        w_key,
        w_value,
    )

    shared = (
        w_query,
        keys,
        values,
        new_keys,
        new_values,
        new_rope,
        prompt_rope_key.T,
        cosine,
        sine,
    )
    total_rows = count * shards
    flops = 4 * total_rows * cached * heads * nope
    if direct:
        sent = call(
            functools.partial(attend_kernel, slots, nope),
            [(count, packed_width)] * shards,
            [VMEM] * (len(shared) + shards),
            "attend",
            flops,
            scratch_shapes=[pltpu.VMEM((total_rows, packed_width), BF16)],
        )(*shared, *blocks)
        got = [sent[0]] + [swap(sent[shards - s], "kv", s) for s in range(1, shards)]
    else:
        step_rows = min(64, total_rows)
        whole = [
            pl.BlockSpec(array.shape, lambda i, rank=array.ndim: (0,) * rank) for array in shared
        ]
        packed = pl.pallas_call(
            functools.partial(attend_kernel, None, nope),
            grid=(total_rows // step_rows,),
            out_shape=jax.ShapeDtypeStruct((total_rows, packed_width), BF16),
            in_specs=whole + [pl.BlockSpec((step_rows, w_qdown.shape[1]), lambda i: (i, 0))],
            out_specs=pl.BlockSpec((step_rows, packed_width), lambda i: (i, 0)),
            name="attend",
            compiler_params=pltpu.CompilerParams(vmem_limit_bytes=24 << 20),
        )(*shared, *blocks)
        got = lax.all_to_all(packed, "kv", split_axis=0, concat_axis=0, tiled=True)
        got = [got[s * count : (s + 1) * count] for s in range(shards)]

    dec_heads, piece_latent, dec_latent, piece_rope, dec_rope = call(
        functools.partial(decode_kernel, nope),
        [(count, heads * value_dim), (count, width), (1, width), (count, rope), (1, rope)],
        [VMEM] * 12,
        "decode",
        4 * count * decode_latent.shape[1] * width * 4,
    )(
        length,
        q_decode,
        w_query,
        w_key,
        w_value,
        decode_latent[0],
        decode_rope_key[0].T,
        dec_latent_rows,
        dec_rope_rows,
        freq,
        new_latent,
        new_rope,
    )

    term = call(
        functools.partial(combine_kernel, heads),
        (2 * count, model),
        [VMEM] * (2 + len(got)),
        "combine",
        2 * 2 * count * heads * value_dim * model,
    )(dec_heads, w_last, *got)
    terms = [term] + [swap(term, "tp", s) for s in range(1, parts)]
    piece_out, decode_out = call(
        add_kernel, [(count, model), (1, model)], [VMEM] * len(terms), "add", 1000
    )(*terms)
    return (piece_out, decode_out, piece_latent, piece_rope, dec_latent, dec_rope)


def solution(mesh):
    rows = P(("dp", "kv"), None)
    cube = P(("dp", "kv"), None, None)
    by_head = P(None, "tp", None)
    in_specs = (
        rows,
        rows,
        rows,
        rows,
        cube,
        cube,
        P(("dp", "kv")),
        P(),
        P(),
        by_head,
        P(),
        P(),
        P(),
        by_head,
        by_head,
        P("tp", None, None),
    )
    return jax.shard_map(
        per_device, mesh=mesh, in_specs=in_specs, out_specs=(rows,) * 6, check_vma=False
    )
```

```python
import functools

import jax
import jax.numpy as jnp
import numpy as np
from jax import lax
from jax.experimental import pallas as pl
from jax.experimental.pallas import tpu as pltpu
from jax.sharding import PartitionSpec as P

LANES = 128
GROUP = 256
MAX_PERMUTES = 8
LOG2_E = 1.4426950408889634
ROPE_BASE = 10000.0
VMEM = pl.BlockSpec(memory_space=pltpu.VMEM)
HBM = pl.BlockSpec(memory_space=pltpu.HBM)
NT = (((1,), (1,)), ((), ()))
F32 = jnp.float32
BF16 = jnp.bfloat16


def dot(a, b):
    return jnp.dot(a, b, preferred_element_type=F32)


def dot_nt(a, b):
    return lax.dot_general(a, b, NT, preferred_element_type=F32)


def lane_index(shape):
    return lax.broadcasted_iota(jnp.int32, shape, len(shape) - 1)


def row_index(shape):
    return lax.broadcasted_iota(jnp.int32, shape, 0)


def rms_scale(values, gain):
    return values * lax.rsqrt(jnp.mean(values * values, axis=-1, keepdims=True) + 1e-06) * gain


def turn(values, cosine, signed_sine, rope):
    half = rope // 2
    swapped = jnp.where(
        lane_index(values.shape) % rope < half,
        pltpu.roll(values, LANES - half, 1),
        pltpu.roll(values, half, 1),
    )
    return values * cosine + swapped * signed_sine


def diagonal(values, count, width):
    owner = lane_index(values.shape) // width
    return jnp.concatenate([jnp.where(owner == j, values, 0.0) for j in range(count)], 0)


def padded(values):
    empty = jnp.zeros((LANES - values.shape[0], values.shape[1]), values.dtype)
    return jnp.concatenate([values, empty], 0)


def spread_rows(row, rows):
    return jnp.broadcast_to(row.astype(F32), (rows, row.shape[1])).astype(row.dtype)


def query_latent_kernel(
    piece_hbm,
    dec_hbm,
    w_hbm,
    gain_hbm,
    out_ref,
    dec_out_ref,
    piece_ref,
    dec_ref,
    gain_ref,
    w_ref,
    sems,
):
    chunks = sems.shape[0] - 3
    depth = w_ref.shape[0] // chunks
    small = []
    for c, (source, target) in enumerate(
        [
            (piece_hbm, piece_ref),
            (dec_hbm, dec_ref),
            (gain_hbm, gain_ref),
        ]
    ):
        small.append(pltpu.make_async_copy(source, target, sems.at[chunks + c]))
        small[-1].start()
    copies = []
    for c in range(chunks):
        part = pl.ds(c * depth, depth)
        copies.append(pltpu.make_async_copy(w_hbm.at[part], w_ref.at[part], sems.at[c]))
        copies[-1].start()
    for copy in small:
        copy.wait()
    piece = piece_ref[...]
    rows = jnp.concatenate([piece, spread_rows(dec_ref[...], piece.shape[0])], 0)
    total = jnp.zeros((rows.shape[0], w_ref.shape[1]), F32)
    for c in range(chunks):
        copies[c].wait()
        part = slice(c * depth, (c + 1) * depth)
        total = total + dot(rows[:, part], w_ref[part, :])
    latent = rms_scale(total, gain_ref[...]).astype(BF16)
    out_ref[...] = latent[: piece.shape[0]]
    dec_out_ref[...] = latent[piece.shape[0] :]


def keys_kernel(
    context,
    lengths_ref,
    piece_ref,
    dec_ref,
    w_ref,
    w_rope_ref,
    gain_ref,
    cos_ref,
    sin_ref,
    freq_ref,
    prompt_ref,
    w_kup_ref,
    w_vup_ref,
    latent_ref,
    dec_latent_ref,
    rope_ref,
    dec_rope_ref,
    key_ref,
    value_ref,
    new_key_ref,
    new_value_ref,
):
    count = piece_ref.shape[0]
    rope = w_rope_ref.shape[0]
    piece = piece_ref[...]
    rows = jnp.concatenate([piece, spread_rows(dec_ref[...], count)], 0)
    latent = rms_scale(dot(rows, w_ref[...]), gain_ref[...]).astype(BF16)
    w_rope = jnp.concatenate([w_rope_ref[...]] * (LANES // rope), 0)
    raw = dot_nt(rows, w_rope)
    index = lax.axis_index("kv")
    own = pl.ds(pl.multiple_of(index * count, count), count)
    new_rope = turn(raw[:count], cos_ref[own, :], sin_ref[own, :], rope).astype(BF16)
    angle = lengths_ref[...] * freq_ref[...]
    sign = jnp.where(lane_index(angle.shape) % rope < rope // 2, -1.0, 1.0)
    dec_rope = turn(raw[count:], jnp.cos(angle), jnp.sin(angle) * sign, rope).astype(BF16)
    latent_ref[...] = latent[:count]
    dec_latent_ref[...] = latent[count:]
    rope_ref[...] = padded(new_rope)
    dec_rope_ref[...] = dec_rope
    w_kup, w_vup = w_kup_ref[...], w_vup_ref[...]
    prompt = prompt_ref[...]
    key_ref[...] = dot_nt(w_kup, prompt).astype(BF16)
    value_ref[...] = dot_nt(prompt, w_vup).astype(BF16)
    new_key_ref[...] = padded(dot_nt(latent[:count], w_kup).astype(BF16))
    new_value_ref[...] = padded(dot_nt(latent[:count], w_vup).astype(BF16))


def split_query_weights(w_ref, nope):
    heads = w_ref.shape[0]
    w_nope = jnp.concatenate([w_ref[h, :nope, :] for h in range(heads)], 0)
    w_rope = jnp.concatenate([w_ref[h, nope:, :] for h in range(heads)], 0)
    return w_nope, w_rope


def attend_kernel(slots, nope, count, *refs):
    (
        w_ref,
        key_ref,
        value_ref,
        new_key_ref,
        new_value_ref,
        new_rope_ref,
        rope_ref,
        cos_ref,
        sin_ref,
    ) = refs[:9]
    index = lax.axis_index("kv")
    part = lax.axis_index("tp")
    if slots:
        shards = len(slots)
        latent_refs, out_refs, out_ref = refs[9 : 9 + shards], refs[9 + shards : -1], refs[-1]
    else:
        latent_refs, out_ref = refs[9:-1], refs[-1]
    heads = w_ref.shape[0]
    rope = w_ref.shape[1] - nope
    latents = jnp.concatenate([ref[...] for ref in latent_refs], 0)
    if slots:
        owners = [lax.rem(index - pick(part, steps) + shards, shards) for steps in slots]
    else:
        first = pl.program_id(0) * (latents.shape[0] // count)
        owners = [first + s for s in range(latents.shape[0] // count)]
    queries = latents.shape[0]
    tables = [pl.ds(pl.multiple_of(owner * count, count), count) for owner in owners]
    cosine = jnp.concatenate([cos_ref[part, :] for part in tables], 0)
    sine = jnp.concatenate([sin_ref[part, :] for part in tables], 0)
    scale = (nope + rope) ** (-0.5)
    per, pair, middle = GROUP // nope, LANES // nope, nope + rope // 2
    old_rope = jnp.concatenate([rope_ref[...]] * (LANES // rope), 0)
    new_rope = new_rope_ref[...]
    row = row_index((count, LANES))
    column = lane_index((count, LANES))
    allowed = jnp.concatenate(
        [
            (column < count) & (index * count + column <= owner * count + row)
            for owner in owners
        ]
        * pair,
        0,
    )
    lane = lane_index((queries, LANES))
    rate = scale * LOG2_E
    stats = jnp.zeros((queries, LANES), F32)
    tiles = key_ref.shape[1] // LANES
    ropes, nopes = [], []
    for g in range(heads // per):
        mine = range(g * per, (g + 1) * per)
        rotary = [w_ref[h, nope:, :] for h in mine]
        for h in mine:
            rotary += [w_ref[h, middle:, :], w_ref[h, nope:middle, :]]
        q_rope = dot_nt(latents, jnp.concatenate(rotary, 0))
        ropes.append(q_rope[:, :LANES] * cosine + q_rope[:, LANES:] * sine)
        q_nope = dot_nt(latents, jnp.concatenate([w_ref[h, :nope, :] for h in mine], 0))
        nopes.append(q_nope.astype(BF16).astype(F32))
    scores = []
    for first in range(0, heads, pair):
        g, p = first // per, first % per // pair
        narrow = slice(first * nope, first * nope + LANES)
        rows = slice(p * pair * queries, (p + 1) * pair * queries)
        query = jnp.concatenate(
            [
                diagonal(nopes[g][:, p * LANES : (p + 1) * LANES], pair, nope),
                diagonal(ropes[g], per, rope)[rows],
            ],
            1,
        ).astype(BF16)
        old = dot(query, jnp.concatenate([key_ref[narrow, :], old_rope], 0))
        new = dot_nt(query, jnp.concatenate([new_key_ref[:, narrow], new_rope], 1))
        new = jnp.where(allowed, new, -1e30)
        scores.append([old[:, t * LANES : (t + 1) * LANES] for t in range(tiles)] + [new])
    weights = []
    for number, pieces in enumerate(scores):
        top = jnp.max(functools.reduce(jnp.maximum, pieces), axis=-1, keepdims=True)
        pieces = [jnp.exp2((piece - top) * rate) for piece in pieces]
        total = jnp.sum(sum(pieces), axis=-1, keepdims=True)
        weights.append([piece.astype(BF16) for piece in pieces])
        for j in range(pair):
            own = slice(j * queries, (j + 1) * queries)
            stats = jnp.where(
                lane % heads == number * pair + j,
                jnp.where(lane < 3 * heads, top[own] * scale, total[own]),
                stats,
            )
    for g in range(heads // per):
        wide = slice(g * GROUP, (g + 1) * GROUP)
        mine = weights[g * per // pair : (g + 1) * per // pair]
        old = jnp.concatenate([jnp.concatenate(pieces[:-1], 1) for pieces in mine], 0)
        new = jnp.concatenate([pieces[-1] for pieces in mine], 0)
        mixed = dot(old, value_ref[:, wide]) + dot(new, new_value_ref[:, wide])
        owner_lane = lane_index((queries, GROUP)) // nope
        kept = jnp.zeros((queries, GROUP), F32)
        for j in range(per):
            kept = jnp.where(owner_lane == j, mixed[j * queries : (j + 1) * queries], kept)
        out_ref[:, wide] = kept.astype(BF16)
    high = stats.astype(BF16).astype(F32)
    rest = stats - high
    middle = rest.astype(BF16).astype(F32)
    piece = (lane // heads) % 3
    stats = jnp.where(piece == 0, high, jnp.where(piece == 1, middle, rest - middle))
    stats = jnp.where(lane < 6 * heads, stats, 0.0)
    out_ref[:, heads * nope :] = stats.astype(BF16)
    if slots:
        for back, ref in enumerate(out_refs):
            places = [[steps[t] for steps in slots].index(back) for t in range(len(slots[0]))]
            ref[...] = block_at(out_ref, pick(part, places), count)


def decode_kernel(
    nope,
    lengths_ref,
    q_ref,
    w_ref,
    w_kup_ref,
    w_vup_ref,
    latent_ref,
    rope_ref,
    new_latent_ref,
    new_rope_ref,
    freq_ref,
    piece_latent_ref,
    piece_rope_ref,
    out_ref,
    latent_out_ref,
    dec_latent_out_ref,
    rope_out_ref,
    dec_rope_out_ref,
):
    heads = w_ref.shape[0]
    rope = w_ref.shape[1] - nope
    latent_out_ref[...] = piece_latent_ref[...]
    dec_latent_out_ref[...] = new_latent_ref[:1, :]
    rope_out_ref[...] = piece_rope_ref[: rope_out_ref.shape[0], :rope]
    dec_rope_out_ref[...] = new_rope_ref[:1, :rope]
    length = lengths_ref[...]
    scale = (nope + rope) ** (-0.5)
    latents = q_ref[...]
    rows = latents.shape[0]
    w_nope, w_rope = split_query_weights(w_ref, nope)
    q_nope = dot_nt(latents, w_nope)
    q_rope = dot_nt(latents, w_rope)
    angle = length * freq_ref[...]
    sign = jnp.where(lane_index(angle.shape) % rope < rope // 2, -1.0, 1.0)
    cosine, sine = jnp.cos(angle), jnp.sin(angle) * sign
    shape = q_nope.shape
    spread = jnp.where(lane_index(shape) // nope == row_index(shape), q_nope, 0.0).astype(BF16)
    absorbed = dot(spread, w_kup_ref[...]).astype(BF16)
    turned = jnp.concatenate(
        [
            turn(q_rope[:, t * LANES : (t + 1) * LANES], cosine, sine, rope)
            for t in range(heads * rope // LANES)
        ],
        1,
    )
    shape = turned.shape
    own_lane = lane_index(shape) // rope == row_index(shape)
    spread_rope = jnp.where(own_lane, turned, 0.0).astype(BF16)
    rope_keys = jnp.concatenate([rope_ref[...]] * heads, 0)
    cached = (dot_nt(absorbed, latent_ref[...]) + dot(spread_rope, rope_keys)) * scale
    cached = jnp.where(lane_index(cached.shape).astype(F32) < length[:, :1], cached, -1e30)
    new_latent = new_latent_ref[...].astype(F32)
    new_rope = jnp.concatenate([new_rope_ref[...].astype(F32)] * (heads * rope // LANES), 1)
    own = (
        jnp.sum(absorbed.astype(F32) * new_latent, axis=-1, keepdims=True)
        + jnp.sum(spread_rope.astype(F32) * new_rope, axis=-1, keepdims=True)
    ) * scale
    top = jnp.maximum(jnp.max(cached, axis=-1, keepdims=True), own)
    cached = jnp.exp(cached - top)
    own = jnp.exp(own - top)
    total = jnp.sum(cached, axis=-1, keepdims=True) + own
    own = (own / total).astype(BF16).astype(F32)
    context = dot((cached / total).astype(BF16), latent_ref[...]) + own * new_latent
    mixed = dot_nt(context.astype(BF16), w_vup_ref[...])
    shape = mixed.shape
    value_dim = w_vup_ref.shape[0] // heads
    mixed = jnp.where(lane_index(shape) // value_dim == row_index(shape), mixed, 0.0)
    total = jnp.sum(mixed, axis=0, keepdims=True)
    out_ref[...] = jnp.broadcast_to(total, out_ref.shape).astype(BF16)


def combine_kernel(heads, dec_ref, w_ref, chosen_ref, *refs):
    count = dec_ref.shape[0]
    got, out_ref = [ref[...] for ref in refs[:-1]], refs[-1]
    width = w_ref.shape[0]
    tails = dot(jnp.concatenate([block[:, width:] for block in got], 0), chosen_ref[...])
    tops = [tails[b * count : (b + 1) * count, :width] for b in range(len(got))]
    totals = [tails[b * count : (b + 1) * count, width:] for b in range(len(got))]
    best = functools.reduce(jnp.maximum, tops)
    factors = [jnp.exp(top - best) for top in tops]
    total = sum(factor * total for factor, total in zip(factors, totals))
    mixed = sum(block[:, :width].astype(F32) * factor for block, factor in zip(got, factors))
    rows = jnp.concatenate([(mixed / total).astype(BF16), dec_ref[...]], 0)
    out_ref[...] = dot(rows, w_ref[...]).astype(BF16)


def chosen_lanes(heads, value_dim):
    lane = np.arange(LANES)[:, None]
    head = np.arange(heads * value_dim)[None, :] // value_dim
    same = lane % heads == head
    tops, totals = same & (lane < 3 * heads), same & (lane >= 3 * heads) & (lane < 6 * heads)
    return np.concatenate([tops, totals], 1).astype(np.float32)


def add_kernel(*refs):
    term_refs, piece_ref, dec_ref = refs[:-2], refs[-2], refs[-1]
    total = sum(ref[...].astype(F32) for ref in term_refs)
    count = piece_ref.shape[0]
    piece_ref[...] = total[:count].astype(BF16)
    dec_ref[...] = total[count : count + 1].astype(BF16)


def call(kernel, outs, in_specs, name, flops, **extra):
    many = isinstance(outs, list)
    shapes = []
    for out in outs if many else [outs]:
        shapes.append(jax.ShapeDtypeStruct(out, BF16))
    limit = extra.pop("limit", 8 << 20)
    specs = [VMEM] * len(shapes)
    return pl.pallas_call(
        kernel,
        out_shape=shapes if many else shapes[0],
        in_specs=in_specs,
        out_specs=specs if many else specs[0],
        name=name,
        compiler_params=pltpu.CompilerParams(vmem_limit_bytes=limit),
        cost_estimate=pl.CostEstimate(flops=flops, bytes_accessed=flops // 64, transcendentals=0),
        **extra,
    )


def ring_pairs(shards, step):
    return [(i, (i + step) % shards) for i in range(shards)]


def mixed_pairs(shards, parts, taken):
    return [
        (i * parts + t, (i + taken[t % len(taken)]) % shards * parts + t)
        for i in range(shards)
        for t in range(parts)
    ]


def swap(values, axis, step):
    return lax.ppermute(values, axis, ring_pairs(lax.axis_size(axis), step))


def gather_plan(shards, parts):
    steps = list(range(1, shards))
    plan = []
    while steps:
        together = parts if parts == 2 and len(steps) >= 2 else 1
        plan.append(steps[:together])
        steps = steps[together:]
    return plan


def slot_steps(plan, parts):
    slots = [[0] * parts]
    for taken in plan:
        for turned in range(len(taken)):
            slots.append([taken[(t + turned) % len(taken)] for t in range(parts)])
    return slots


def pick(index, values):
    chosen = jnp.int32(values[0])
    for i, value in enumerate(values):
        if value != values[0]:
            chosen = jnp.where(index == i, value, chosen)
    return chosen


def block_at(ref, number, count):
    return ref[pl.ds(pl.multiple_of(number * count, count), count), :]


def in_hbm(array):
    return pltpu.with_memory_space_constraint(array, pltpu.HBM)


def rope_tables(context, rows, rope):
    half = rope // 2
    inverse = ROPE_BASE ** (-np.arange(half, dtype=np.float32) * 2.0 / rope)
    inverse = inverse.astype(np.float32)
    lanes = np.tile(inverse, LANES // half)[None, :]
    angle = (context + np.arange(rows, dtype=np.float32))[:, None] * lanes
    sign = np.where(np.arange(LANES) % rope < half, -1.0, 1.0)
    return (
        np.cos(angle).astype(np.float32),
        (np.sin(angle) * sign).astype(np.float32),
        lanes.astype(np.float32),
    )


def per_device(
    piece_rows,
    decode_rows,
    prompt_latent,
    prompt_rope_key,
    decode_latent,
    decode_rope_key,
    dec_lengths,
    w_qdown,
    q_gain,
    w_qup,
    w_kvdown,
    w_krope,
    kv_gain,
    w_kup,
    w_vup,
    w_out,
):
    shards, parts = lax.axis_size("kv"), lax.axis_size("tp")
    count, model = piece_rows.shape
    cached, width = prompt_latent.shape
    context = cached * shards
    heads, nope = w_kup.shape[1:]
    value_dim = w_vup.shape[2]
    rope = w_krope.shape[1]
    assert decode_rows.shape[0] == 1
    cosine, sine, freq = rope_tables(context, count * shards, rope)
    w_query = jnp.transpose(w_qup, (1, 2, 0))
    w_key = jnp.transpose(w_kup, (1, 2, 0)).reshape(heads * nope, width)
    w_value = jnp.transpose(w_vup, (1, 2, 0)).reshape(heads * value_dim, width)
    w_last = w_out.reshape(heads * value_dim, model)
    packed_width = heads * value_dim + LANES

    q_latent, q_decode = call(
        query_latent_kernel,
        [(count, w_qdown.shape[1]), (count, w_qdown.shape[1])],
        [HBM] * 4,
        "query_latent",
        2 * 2 * count * model * w_qdown.shape[1] * 100,
        scratch_shapes=[
            pltpu.VMEM(piece_rows.shape, BF16),
            pltpu.VMEM(decode_rows.shape, BF16),
            pltpu.VMEM((1, q_gain.shape[0]), F32),
            pltpu.VMEM(w_qdown.shape, BF16),
            pltpu.SemaphoreType.DMA((4 + 3,)),
        ],
    )(*[in_hbm(array) for array in (piece_rows, decode_rows, w_qdown, q_gain[None, :])])

    length = jnp.broadcast_to(dec_lengths.astype(F32)[:, None], (1, LANES))
    direct = shards <= MAX_PERMUTES
    if direct:
        plan = gather_plan(shards, parts)
        slots = slot_steps(plan, parts)
        blocks = [q_latent]
        for taken in plan:
            blocks.append(lax.ppermute(q_latent, ("kv", "tp"), mixed_pairs(shards, parts, taken)))
            if len(taken) > 1:
                blocks.append(swap(blocks[-1], "tp", 1))
    else:
        blocks = [lax.all_gather(q_latent, "kv", axis=0, tiled=True)]

    new_latent, dec_latent_rows, new_rope, dec_rope_rows, keys, values, new_keys, new_values = call(
        functools.partial(keys_kernel, context),
        [
            (count, width),
            (count, width),
            (LANES, LANES),
            (count, LANES),
            (heads * nope, cached),
            (cached, heads * value_dim),
            (LANES, heads * nope),
            (LANES, heads * value_dim),
        ],
        [VMEM] * 12,
        "keys",
        4 * cached * width * heads * nope,
    )(
        length,
        piece_rows,
        decode_rows,
        w_kvdown,
        w_krope.T,
        kv_gain[None, :],
        cosine,
        sine,
        freq,
        prompt_latent,
        w_key,
        w_value,
    )

    shared = (
        w_query,
        keys,
        values,
        new_keys,
        new_values,
        new_rope,
        prompt_rope_key.T,
        cosine,
        sine,
    )
    total_rows = count * shards
    flops = 4 * total_rows * cached * heads * nope
    if direct:
        sent = call(
            functools.partial(attend_kernel, slots, nope, count),
            [(count, packed_width)] * shards,
            [VMEM] * (len(shared) + shards),
            "attend",
            flops,
            scratch_shapes=[pltpu.VMEM((total_rows, packed_width), BF16)],
        )(*shared, *blocks)
        got = [sent[0]] + [swap(sent[shards - s], "kv", s) for s in range(1, shards)]
    else:
        step_rows = min(64, total_rows)
        whole = [
            pl.BlockSpec(array.shape, lambda i, rank=array.ndim: (0,) * rank) for array in shared
        ]
        packed = pl.pallas_call(
            functools.partial(attend_kernel, None, nope, count),
            grid=(total_rows // step_rows,),
            out_shape=jax.ShapeDtypeStruct((total_rows, packed_width), BF16),
            in_specs=whole + [pl.BlockSpec((step_rows, w_qdown.shape[1]), lambda i: (i, 0))],
            out_specs=pl.BlockSpec((step_rows, packed_width), lambda i: (i, 0)),
            name="attend",
            compiler_params=pltpu.CompilerParams(vmem_limit_bytes=24 << 20),
        )(*shared, *blocks)
        got = lax.all_to_all(packed, "kv", split_axis=0, concat_axis=0, tiled=True)
        got = [got[s * count : (s + 1) * count] for s in range(shards)]

    dec_heads, piece_latent, dec_latent, piece_rope, dec_rope = call(
        functools.partial(decode_kernel, nope),
        [(count, heads * value_dim), (count, width), (1, width), (count, rope), (1, rope)],
        [VMEM] * 12,
        "decode",
        4 * count * decode_latent.shape[1] * width * 4,
    )(
        length,
        q_decode,
        w_query,
        w_key,
        w_value,
        decode_latent[0],
        decode_rope_key[0].T,
        dec_latent_rows,
        dec_rope_rows,
        freq,
        new_latent,
        new_rope,
    )

    term = call(
        functools.partial(combine_kernel, heads),
        (2 * count, model),
        [VMEM] * (3 + len(got)),
        "combine",
        2 * 2 * count * heads * value_dim * model,
    )(dec_heads, w_last, jnp.asarray(chosen_lanes(heads, value_dim), BF16), *got)
    terms = [term] + [swap(term, "tp", s) for s in range(1, parts)]
    piece_out, decode_out = call(
        add_kernel, [(count, model), (1, model)], [VMEM] * len(terms), "add", 1000
    )(*terms)
    return (piece_out, decode_out, piece_latent, piece_rope, dec_latent, dec_rope)


def solution(mesh):
    rows = P(("dp", "kv"), None)
    cube = P(("dp", "kv"), None, None)
    by_head = P(None, "tp", None)
    in_specs = (
        rows,
        rows,
        rows,
        rows,
        cube,
        cube,
        P(("dp", "kv")),
        P(),
        P(),
        by_head,
        P(),
        P(),
        P(),
        by_head,
        by_head,
        P("tp", None, None),
    )
    return jax.shard_map(
        per_device, mesh=mesh, in_specs=in_specs, out_specs=(rows,) * 6, check_vma=False
    )
```

```python
import functools

import jax
import jax.numpy as jnp
import numpy as np
from jax import lax
from jax.experimental import pallas as pl
from jax.experimental.pallas import tpu as pltpu
from jax.sharding import PartitionSpec as P

LANES = 128
GROUP = 256
MAX_PERMUTES = 8
LOG2_E = 1.4426950408889634
ROPE_BASE = 10000.0
CUTS = (0, 2, 4, 6, 7, 8)
VMEM = pl.BlockSpec(memory_space=pltpu.VMEM)
HBM = pl.BlockSpec(memory_space=pltpu.HBM)
NT = (((1,), (1,)), ((), ()))
F32 = jnp.float32
BF16 = jnp.bfloat16


def dot(a, b):
    return jnp.dot(a, b, preferred_element_type=F32)


def dot_nt(a, b):
    return lax.dot_general(a, b, NT, preferred_element_type=F32)


def lane_index(shape):
    return lax.broadcasted_iota(jnp.int32, shape, len(shape) - 1)


def row_index(shape):
    return lax.broadcasted_iota(jnp.int32, shape, 0)


def rms_scale(values, gain):
    return values * lax.rsqrt(jnp.mean(values * values, axis=-1, keepdims=True) + 1e-06) * gain


def turn(values, cosine, signed_sine, rope):
    half = rope // 2
    swapped = jnp.where(
        lane_index(values.shape) % rope < half,
        pltpu.roll(values, LANES - half, 1),
        pltpu.roll(values, half, 1),
    )
    return values * cosine + swapped * signed_sine


def diagonal(values, count, width):
    owner = lane_index(values.shape) // width
    return jnp.concatenate([jnp.where(owner == j, values, 0.0) for j in range(count)], 0)


def padded(values):
    empty = jnp.zeros((LANES - values.shape[0], values.shape[1]), values.dtype)
    return jnp.concatenate([values, empty], 0)


def spread_rows(row, rows):
    return jnp.broadcast_to(row.astype(F32), (rows, row.shape[1])).astype(row.dtype)


def query_latent_kernel(
    piece_hbm,
    dec_hbm,
    w_hbm,
    gain_hbm,
    out_ref,
    dec_out_ref,
    piece_ref,
    dec_ref,
    gain_ref,
    w_ref,
    sems,
):
    depth = w_ref.shape[0] // CUTS[-1]
    parts = [slice(a * depth, b * depth) for a, b in zip(CUTS[:-1], CUTS[1:])]
    pairs = [(piece_hbm, piece_ref), (dec_hbm, dec_ref), (gain_hbm, gain_ref)]
    small = len(pairs)
    pairs += [(w_hbm.at[part], w_ref.at[part]) for part in parts]
    copies = []
    for c, (source, target) in enumerate(pairs):
        copies.append(pltpu.make_async_copy(source, target, sems.at[c]))
        copies[-1].start()
    for copy in copies[:small]:
        copy.wait()
    piece = piece_ref[...]
    rows = jnp.concatenate([piece, spread_rows(dec_ref[...], piece.shape[0])], 0)
    total = jnp.zeros((rows.shape[0], w_ref.shape[1]), F32)
    for copy, part in zip(copies[small:], parts):
        copy.wait()
        total = total + dot(rows[:, part], w_ref[part, :])
    latent = rms_scale(total, gain_ref[...]).astype(BF16)
    out_ref[...] = latent[: piece.shape[0]]
    dec_out_ref[...] = latent[piece.shape[0] :]


def turn_weights(nope, w_ref, nope_out_ref, rope_out_ref):
    heads = w_ref.shape[0]
    middle = (nope + w_ref.shape[1]) // 2
    per = GROUP // nope
    w_nope = [w_ref[h, :nope, :] for h in range(heads)]
    rotary = []
    for g in range(heads // per):
        mine = range(g * per, (g + 1) * per)
        rotary += [w_ref[h, nope:, :] for h in mine]
        for h in mine:
            rotary += [w_ref[h, middle:, :], w_ref[h, nope:middle, :]]
    nope_out_ref[...] = jnp.concatenate(w_nope, 0).T
    rope_out_ref[...] = jnp.concatenate(rotary, 0).T


def keys_kernel(
    context,
    nope,
    lengths_ref,
    piece_ref,
    dec_ref,
    w_ref,
    w_rope_ref,
    gain_ref,
    cos_ref,
    sin_ref,
    freq_ref,
    prompt_ref,
    w_kup_ref,
    w_vup_ref,
    w_query_ref,
    latent_ref,
    dec_latent_ref,
    rope_ref,
    dec_rope_ref,
    key_ref,
    value_ref,
    new_key_ref,
    new_value_ref,
    w_nope_ref,
    w_turned_ref,
):
    turn_weights(nope, w_query_ref, w_nope_ref, w_turned_ref)
    count = piece_ref.shape[0]
    rope = w_rope_ref.shape[0]
    piece = piece_ref[...]
    rows = jnp.concatenate([piece, spread_rows(dec_ref[...], count)], 0)
    latent = rms_scale(dot(rows, w_ref[...]), gain_ref[...]).astype(BF16)
    w_rope = jnp.concatenate([w_rope_ref[...]] * (LANES // rope), 0)
    raw = dot_nt(rows, w_rope)
    index = lax.axis_index("kv")
    own = pl.ds(pl.multiple_of(index * count, count), count)
    new_rope = turn(raw[:count], cos_ref[own, :], sin_ref[own, :], rope).astype(BF16)
    angle = lengths_ref[...] * freq_ref[...]
    sign = jnp.where(lane_index(angle.shape) % rope < rope // 2, -1.0, 1.0)
    dec_rope = turn(raw[count:], jnp.cos(angle), jnp.sin(angle) * sign, rope).astype(BF16)
    latent_ref[...] = latent[:count]
    dec_latent_ref[...] = latent[count:]
    rope_ref[...] = new_rope
    dec_rope_ref[...] = dec_rope
    w_kup, w_vup = w_kup_ref[...], w_vup_ref[...]
    prompt = prompt_ref[...]
    key_ref[...] = dot_nt(w_kup, prompt).astype(BF16)
    value_ref[...] = dot_nt(prompt, w_vup).astype(BF16)
    new_key_ref[...] = dot_nt(latent[:count], w_kup).astype(BF16)
    new_value_ref[...] = padded(dot_nt(latent[:count], w_vup).astype(BF16))


def split_query_weights(w_ref, nope):
    heads = w_ref.shape[0]
    w_nope = jnp.concatenate([w_ref[h, :nope, :] for h in range(heads)], 0)
    w_rope = jnp.concatenate([w_ref[h, nope:, :] for h in range(heads)], 0)
    return w_nope, w_rope


def attend_kernel(slots, nope, count, *refs):
    (
        w_nope_ref,
        w_rope_ref,
        key_ref,
        value_ref,
        new_key_ref,
        new_value_ref,
        new_rope_ref,
        rope_ref,
        cos_ref,
        sin_ref,
    ) = refs[:10]
    index = lax.axis_index("kv")
    part = lax.axis_index("tp")
    if slots:
        shards = len(slots)
        latent_refs, out_refs, out_ref = refs[10 : 10 + shards], refs[10 + shards : -1], refs[-1]
    else:
        latent_refs, out_ref = refs[10:-1], refs[-1]
    heads = w_nope_ref.shape[1] // nope
    rope = rope_ref.shape[0]
    latents = jnp.concatenate([ref[...] for ref in latent_refs], 0)
    if slots:
        owners = [lax.rem(index - pick(part, steps) + shards, shards) for steps in slots]
    else:
        first = pl.program_id(0) * (latents.shape[0] // count)
        owners = [first + s for s in range(latents.shape[0] // count)]
    queries = latents.shape[0]
    tables = [pl.ds(pl.multiple_of(owner * count, count), count) for owner in owners]
    cosine = jnp.concatenate([cos_ref[part, :] for part in tables], 0)
    sine = jnp.concatenate([sin_ref[part, :] for part in tables], 0)
    scale = (nope + rope) ** (-0.5)
    per, pair = GROUP // nope, LANES // nope
    old_rope = jnp.concatenate([rope_ref[...]] * (LANES // rope), 0)
    new_rope = new_rope_ref[...]
    row = row_index((count, LANES))
    column = lane_index((count, LANES))
    allowed = jnp.concatenate(
        [
            (column < count) & (index * count + column <= owner * count + row)
            for owner in owners
        ]
        * pair,
        0,
    )
    lane = lane_index((queries, LANES))
    rate = scale * LOG2_E
    stats = jnp.zeros((queries, LANES), F32)
    tiles = key_ref.shape[1] // LANES
    ropes, nopes = [], []
    for g in range(heads // per):
        wide = slice(g * GROUP, (g + 1) * GROUP)
        q_rope = dot(latents, w_rope_ref[:, wide])
        ropes.append(q_rope[:, :LANES] * cosine + q_rope[:, LANES:] * sine)
        nopes.append(dot(latents, w_nope_ref[:, wide]).astype(BF16).astype(F32))
    scores = []
    for first in range(0, heads, pair):
        g, p = first // per, first % per // pair
        narrow = slice(first * nope, first * nope + LANES)
        rows = slice(p * pair * queries, (p + 1) * pair * queries)
        query = jnp.concatenate(
            [
                diagonal(nopes[g][:, p * LANES : (p + 1) * LANES], pair, nope),
                diagonal(ropes[g], per, rope)[rows],
            ],
            1,
        ).astype(BF16)
        old = dot(query, jnp.concatenate([key_ref[narrow, :], old_rope], 0))
        new = dot_nt(query, jnp.concatenate([new_key_ref[:, narrow], new_rope], 1))
        empty = jnp.zeros((new.shape[0], LANES - count), F32)
        new = jnp.where(allowed, jnp.concatenate([new, empty], 1), -1e30)
        scores.append([old[:, t * LANES : (t + 1) * LANES] for t in range(tiles)] + [new])
    weights = []
    for number, pieces in enumerate(scores):
        top = jnp.max(functools.reduce(jnp.maximum, pieces), axis=-1, keepdims=True)
        pieces = [jnp.exp2((piece - top) * rate) for piece in pieces]
        total = jnp.sum(sum(pieces), axis=-1, keepdims=True)
        weights.append([piece.astype(BF16) for piece in pieces])
        for j in range(pair):
            own = slice(j * queries, (j + 1) * queries)
            stats = jnp.where(
                lane % heads == number * pair + j,
                jnp.where(lane < 3 * heads, top[own] * scale, total[own]),
                stats,
            )
    for g in range(heads // per):
        wide = slice(g * GROUP, (g + 1) * GROUP)
        mine = weights[g * per // pair : (g + 1) * per // pair]
        old = jnp.concatenate([jnp.concatenate(pieces[:-1], 1) for pieces in mine], 0)
        new = jnp.concatenate([pieces[-1] for pieces in mine], 0)
        mixed = dot(old, value_ref[:, wide]) + dot(new, new_value_ref[:, wide])
        owner_lane = lane_index((queries, GROUP)) // nope
        kept = jnp.zeros((queries, GROUP), F32)
        for j in range(per):
            kept = jnp.where(owner_lane == j, mixed[j * queries : (j + 1) * queries], kept)
        out_ref[:, wide] = kept.astype(BF16)
    high = stats.astype(BF16).astype(F32)
    rest = stats - high
    middle = rest.astype(BF16).astype(F32)
    piece = (lane // heads) % 3
    stats = jnp.where(piece == 0, high, jnp.where(piece == 1, middle, rest - middle))
    stats = jnp.where(lane < 6 * heads, stats, 0.0)
    out_ref[:, heads * nope :] = stats.astype(BF16)
    if slots:
        for back, ref in enumerate(out_refs):
            places = [[steps[t] for steps in slots].index(back) for t in range(len(slots[0]))]
            ref[...] = block_at(out_ref, pick(part, places), count)


def decode_kernel(
    nope,
    lengths_ref,
    q_ref,
    w_ref,
    w_kup_ref,
    w_vup_ref,
    latent_ref,
    rope_ref,
    new_latent_ref,
    new_rope_ref,
    freq_ref,
    piece_latent_ref,
    piece_rope_ref,
    out_ref,
    latent_out_ref,
    dec_latent_out_ref,
    rope_out_ref,
    dec_rope_out_ref,
):
    heads = w_ref.shape[0]
    rope = w_ref.shape[1] - nope
    latent_out_ref[...] = piece_latent_ref[...]
    dec_latent_out_ref[...] = new_latent_ref[:1, :]
    rope_out_ref[...] = piece_rope_ref[: rope_out_ref.shape[0], :rope]
    dec_rope_out_ref[...] = new_rope_ref[:1, :rope]
    length = lengths_ref[...]
    scale = (nope + rope) ** (-0.5)
    latents = q_ref[...]
    rows = latents.shape[0]
    w_nope, w_rope = split_query_weights(w_ref, nope)
    q_nope = dot_nt(latents, w_nope)
    q_rope = dot_nt(latents, w_rope)
    angle = length * freq_ref[...]
    sign = jnp.where(lane_index(angle.shape) % rope < rope // 2, -1.0, 1.0)
    cosine, sine = jnp.cos(angle), jnp.sin(angle) * sign
    shape = q_nope.shape
    spread = jnp.where(lane_index(shape) // nope == row_index(shape), q_nope, 0.0).astype(BF16)
    absorbed = dot(spread, w_kup_ref[...]).astype(BF16)
    turned = jnp.concatenate(
        [
            turn(q_rope[:, t * LANES : (t + 1) * LANES], cosine, sine, rope)
            for t in range(heads * rope // LANES)
        ],
        1,
    )
    shape = turned.shape
    own_lane = lane_index(shape) // rope == row_index(shape)
    spread_rope = jnp.where(own_lane, turned, 0.0).astype(BF16)
    rope_keys = jnp.concatenate([rope_ref[...]] * heads, 0)
    cached = (dot_nt(absorbed, latent_ref[...]) + dot(spread_rope, rope_keys)) * scale
    cached = jnp.where(lane_index(cached.shape).astype(F32) < length[:, :1], cached, -1e30)
    new_latent = new_latent_ref[...].astype(F32)
    new_rope = jnp.concatenate([new_rope_ref[...].astype(F32)] * (heads * rope // LANES), 1)
    own = (
        jnp.sum(absorbed.astype(F32) * new_latent, axis=-1, keepdims=True)
        + jnp.sum(spread_rope.astype(F32) * new_rope, axis=-1, keepdims=True)
    ) * scale
    top = jnp.maximum(jnp.max(cached, axis=-1, keepdims=True), own)
    cached = jnp.exp(cached - top)
    own = jnp.exp(own - top)
    total = jnp.sum(cached, axis=-1, keepdims=True) + own
    own = (own / total).astype(BF16).astype(F32)
    context = dot((cached / total).astype(BF16), latent_ref[...]) + own * new_latent
    mixed = dot_nt(context.astype(BF16), w_vup_ref[...])
    shape = mixed.shape
    value_dim = w_vup_ref.shape[0] // heads
    mixed = jnp.where(lane_index(shape) // value_dim == row_index(shape), mixed, 0.0)
    total = jnp.sum(mixed, axis=0, keepdims=True)
    out_ref[...] = jnp.broadcast_to(total, out_ref.shape).astype(BF16)


def combine_kernel(heads, dec_ref, w_ref, chosen_ref, *refs):
    count = dec_ref.shape[0]
    got, out_ref = [ref[...] for ref in refs[:-1]], refs[-1]
    width = w_ref.shape[0]
    tails = dot(jnp.concatenate([block[:, width:] for block in got], 0), chosen_ref[...])
    tops = [tails[b * count : (b + 1) * count, :width] for b in range(len(got))]
    totals = [tails[b * count : (b + 1) * count, width:] for b in range(len(got))]
    best = functools.reduce(jnp.maximum, tops)
    factors = [jnp.exp(top - best) for top in tops]
    total = sum(factor * total for factor, total in zip(factors, totals))
    mixed = sum(block[:, :width].astype(F32) * factor for block, factor in zip(got, factors))
    rows = jnp.concatenate([(mixed / total).astype(BF16), dec_ref[...]], 0)
    out_ref[...] = dot(rows, w_ref[...])[: out_ref.shape[0]].astype(BF16)


def chosen_lanes(heads, value_dim):
    lane = np.arange(LANES)[:, None]
    head = np.arange(heads * value_dim)[None, :] // value_dim
    same = lane % heads == head
    tops, totals = same & (lane < 3 * heads), same & (lane >= 3 * heads) & (lane < 6 * heads)
    return np.concatenate([tops, totals], 1).astype(np.float32)


def add_kernel(*refs):
    term_refs, piece_ref, dec_ref = refs[:-2], refs[-2], refs[-1]
    total = sum(ref[...].astype(F32) for ref in term_refs)
    count = piece_ref.shape[0]
    piece_ref[...] = total[:count].astype(BF16)
    dec_ref[...] = total[count : count + 1].astype(BF16)


def call(kernel, outs, in_specs, name, flops, **extra):
    many = isinstance(outs, list)
    shapes = []
    for out in outs if many else [outs]:
        shapes.append(jax.ShapeDtypeStruct(out, BF16))
    limit = extra.pop("limit", 8 << 20)
    specs = [VMEM] * len(shapes)
    return pl.pallas_call(
        kernel,
        out_shape=shapes if many else shapes[0],
        in_specs=in_specs,
        out_specs=specs if many else specs[0],
        name=name,
        compiler_params=pltpu.CompilerParams(vmem_limit_bytes=limit),
        cost_estimate=pl.CostEstimate(flops=flops, bytes_accessed=flops // 64, transcendentals=0),
        **extra,
    )


def ring_pairs(shards, step):
    return [(i, (i + step) % shards) for i in range(shards)]


def mixed_pairs(shards, parts, taken):
    return [
        (i * parts + t, (i + taken[t % len(taken)]) % shards * parts + t)
        for i in range(shards)
        for t in range(parts)
    ]


def swap(values, axis, step):
    return lax.ppermute(values, axis, ring_pairs(lax.axis_size(axis), step))


def gather_plan(shards, parts):
    steps = list(range(1, shards))
    plan = []
    while steps:
        together = parts if parts == 2 and len(steps) >= 2 else 1
        plan.append(steps[:together])
        steps = steps[together:]
    return plan


def slot_steps(plan, parts):
    slots = [[0] * parts]
    for taken in plan:
        for turned in range(len(taken)):
            slots.append([taken[(t + turned) % len(taken)] for t in range(parts)])
    return slots


def pick(index, values):
    chosen = jnp.int32(values[0])
    for i, value in enumerate(values):
        if value != values[0]:
            chosen = jnp.where(index == i, value, chosen)
    return chosen


def block_at(ref, number, count):
    return ref[pl.ds(pl.multiple_of(number * count, count), count), :]


def in_hbm(array):
    return pltpu.with_memory_space_constraint(array, pltpu.HBM)


def rope_tables(context, rows, rope):
    half = rope // 2
    inverse = ROPE_BASE ** (-np.arange(half, dtype=np.float32) * 2.0 / rope)
    inverse = inverse.astype(np.float32)
    lanes = np.tile(inverse, LANES // half)[None, :]
    angle = (context + np.arange(rows, dtype=np.float32))[:, None] * lanes
    sign = np.where(np.arange(LANES) % rope < half, -1.0, 1.0)
    return (
        np.cos(angle).astype(np.float32),
        (np.sin(angle) * sign).astype(np.float32),
        lanes.astype(np.float32),
    )


def per_device(
    piece_rows,
    decode_rows,
    prompt_latent,
    prompt_rope_key,
    decode_latent,
    decode_rope_key,
    dec_lengths,
    w_qdown,
    q_gain,
    w_qup,
    w_kvdown,
    w_krope,
    kv_gain,
    w_kup,
    w_vup,
    w_out,
):
    shards, parts = lax.axis_size("kv"), lax.axis_size("tp")
    count, model = piece_rows.shape
    cached, width = prompt_latent.shape
    context = cached * shards
    heads, nope = w_kup.shape[1:]
    value_dim = w_vup.shape[2]
    rope = w_krope.shape[1]
    assert decode_rows.shape[0] == 1
    cosine, sine, freq = rope_tables(context, count * shards, rope)
    w_query = jnp.transpose(w_qup, (1, 2, 0))
    w_key = jnp.transpose(w_kup, (1, 2, 0)).reshape(heads * nope, width)
    w_value = jnp.transpose(w_vup, (1, 2, 0)).reshape(heads * value_dim, width)
    w_last = w_out.reshape(heads * value_dim, model)
    packed_width = heads * value_dim + LANES

    q_latent, q_decode = call(
        query_latent_kernel,
        [(count, w_qdown.shape[1]), (count, w_qdown.shape[1])],
        [HBM] * 4,
        "query_latent",
        2 * 2 * count * model * w_qdown.shape[1] * 100,
        scratch_shapes=[
            pltpu.VMEM(piece_rows.shape, BF16),
            pltpu.VMEM(decode_rows.shape, BF16),
            pltpu.VMEM((1, q_gain.shape[0]), F32),
            pltpu.VMEM(w_qdown.shape, BF16),
            pltpu.SemaphoreType.DMA((len(CUTS) - 1 + 3,)),
        ],
    )(*[in_hbm(array) for array in (piece_rows, decode_rows, w_qdown, q_gain[None, :])])

    length = jnp.broadcast_to(dec_lengths.astype(F32)[:, None], (1, LANES))
    direct = shards <= MAX_PERMUTES
    if direct:
        plan = gather_plan(shards, parts)
        slots = slot_steps(plan, parts)
        blocks = [q_latent]
        for taken in plan:
            blocks.append(lax.ppermute(q_latent, ("kv", "tp"), mixed_pairs(shards, parts, taken)))
            if len(taken) > 1:
                blocks.append(swap(blocks[-1], "tp", 1))
    else:
        blocks = [lax.all_gather(q_latent, "kv", axis=0, tiled=True)]

    (
        new_latent,
        dec_latent_rows,
        new_rope,
        dec_rope_rows,
        keys,
        values,
        new_keys,
        new_values,
        w_nope,
        w_rope,
    ) = call(
        functools.partial(keys_kernel, context, nope),
        [
            (count, width),
            (count, width),
            (count, LANES),
            (count, LANES),
            (heads * nope, cached),
            (cached, heads * value_dim),
            (count, heads * nope),
            (LANES, heads * value_dim),
            (w_qup.shape[0], heads * nope),
            (w_qup.shape[0], heads * rope * 2),
        ],
        [VMEM] * 13,
        "keys",
        4 * cached * width * heads * nope,
    )(
        length,
        piece_rows,
        decode_rows,
        w_kvdown,
        w_krope.T,
        kv_gain[None, :],
        cosine,
        sine,
        freq,
        prompt_latent,
        w_key,
        w_value,
        w_query,
    )

    shared = (
        w_nope,
        w_rope,
        keys,
        values,
        new_keys,
        new_values,
        new_rope,
        prompt_rope_key.T,
        cosine,
        sine,
    )
    total_rows = count * shards
    flops = 4 * total_rows * cached * heads * nope
    if direct:
        sent = call(
            functools.partial(attend_kernel, slots, nope, count),
            [(count, packed_width)] * shards,
            [VMEM] * (len(shared) + shards),
            "attend",
            flops,
            scratch_shapes=[pltpu.VMEM((total_rows, packed_width), BF16)],
        )(*shared, *blocks)
        got = [sent[0]] + [swap(sent[shards - s], "kv", s) for s in range(1, shards)]
    else:
        step_rows = min(64, total_rows)
        whole = [
            pl.BlockSpec(array.shape, lambda i, rank=array.ndim: (0,) * rank) for array in shared
        ]
        packed = pl.pallas_call(
            functools.partial(attend_kernel, None, nope, count),
            grid=(total_rows // step_rows,),
            out_shape=jax.ShapeDtypeStruct((total_rows, packed_width), BF16),
            in_specs=whole + [pl.BlockSpec((step_rows, w_qdown.shape[1]), lambda i: (i, 0))],
            out_specs=pl.BlockSpec((step_rows, packed_width), lambda i: (i, 0)),
            name="attend",
            compiler_params=pltpu.CompilerParams(vmem_limit_bytes=24 << 20),
        )(*shared, *blocks)
        got = lax.all_to_all(packed, "kv", split_axis=0, concat_axis=0, tiled=True)
        got = [got[s * count : (s + 1) * count] for s in range(shards)]

    dec_heads, piece_latent, dec_latent, piece_rope, dec_rope = call(
        functools.partial(decode_kernel, nope),
        [(count, heads * value_dim), (count, width), (1, width), (count, rope), (1, rope)],
        [VMEM] * 12,
        "decode",
        4 * count * decode_latent.shape[1] * width * 4,
    )(
        length,
        q_decode,
        w_query,
        w_key,
        w_value,
        decode_latent[0],
        decode_rope_key[0].T,
        dec_latent_rows,
        dec_rope_rows,
        freq,
        new_latent,
        new_rope,
    )

    term = call(
        functools.partial(combine_kernel, heads),
        (count + 8, model),
        [VMEM] * (3 + len(got)),
        "combine",
        2 * 2 * count * heads * value_dim * model,
    )(dec_heads, w_last, jnp.asarray(chosen_lanes(heads, value_dim), BF16), *got)
    terms = [term] + [swap(term, "tp", s) for s in range(1, parts)]
    piece_out, decode_out = call(
        add_kernel, [(count, model), (1, model)], [VMEM] * len(terms), "add", 1000
    )(*terms)
    return (piece_out, decode_out, piece_latent, piece_rope, dec_latent, dec_rope)


def solution(mesh):
    rows = P(("dp", "kv"), None)
    cube = P(("dp", "kv"), None, None)
    by_head = P(None, "tp", None)
    in_specs = (
        rows,
        rows,
        rows,
        rows,
        cube,
        cube,
        P(("dp", "kv")),
        P(),
        P(),
        by_head,
        P(),
        P(),
        P(),
        by_head,
        by_head,
        P("tp", None, None),
    )
    return jax.shard_map(
        per_device, mesh=mesh, in_specs=in_specs, out_specs=(rows,) * 6, check_vma=False
    )
```

```python
import functools

import jax
import jax.numpy as jnp
import numpy as np
from jax import lax
from jax.experimental import pallas as pl
from jax.experimental.pallas import tpu as pltpu
from jax.sharding import PartitionSpec as P

LANES = 128
GROUP = 256
MAX_PERMUTES = 8
LOG2_E = 1.4426950408889634
ROPE_BASE = 10000.0
CUTS = (0, 1, 2, 3, 4, 5, 6, 7, 8)
VMEM = pl.BlockSpec(memory_space=pltpu.VMEM)
HBM = pl.BlockSpec(memory_space=pltpu.HBM)
NT = (((1,), (1,)), ((), ()))
F32 = jnp.float32
BF16 = jnp.bfloat16


def dot(a, b):
    return jnp.dot(a, b, preferred_element_type=F32)


def dot_nt(a, b):
    return lax.dot_general(a, b, NT, preferred_element_type=F32)


def lane_index(shape):
    return lax.broadcasted_iota(jnp.int32, shape, len(shape) - 1)


def row_index(shape):
    return lax.broadcasted_iota(jnp.int32, shape, 0)


def rms_scale(values, gain):
    return values * lax.rsqrt(jnp.mean(values * values, axis=-1, keepdims=True) + 1e-06) * gain


def turn(values, cosine, signed_sine, rope):
    half = rope // 2
    swapped = jnp.where(
        lane_index(values.shape) % rope < half,
        pltpu.roll(values, LANES - half, 1),
        pltpu.roll(values, half, 1),
    )
    return values * cosine + swapped * signed_sine


def diagonal(values, count, width):
    owner = lane_index(values.shape) // width
    return jnp.concatenate([jnp.where(owner == j, values, 0.0) for j in range(count)], 0)


def padded(values):
    empty = jnp.zeros((LANES - values.shape[0], values.shape[1]), values.dtype)
    return jnp.concatenate([values, empty], 0)


def spread_rows(row, rows):
    return jnp.broadcast_to(row.astype(F32), (rows, row.shape[1])).astype(row.dtype)


def query_latent_kernel(
    piece_hbm,
    dec_hbm,
    w_hbm,
    gain_hbm,
    out_ref,
    dec_out_ref,
    piece_ref,
    dec_ref,
    gain_ref,
    w_ref,
    sems,
):
    depth = w_ref.shape[0] // CUTS[-1]
    parts = [slice(a * depth, b * depth) for a, b in zip(CUTS[:-1], CUTS[1:])]
    pairs = [(piece_hbm, piece_ref), (dec_hbm, dec_ref), (gain_hbm, gain_ref)]
    small = len(pairs)
    pairs += [(w_hbm.at[part], w_ref.at[part]) for part in parts]
    copies = []
    for c, (source, target) in enumerate(pairs):
        copies.append(pltpu.make_async_copy(source, target, sems.at[c]))
        copies[-1].start()
    for copy in copies[:small]:
        copy.wait()
    piece = piece_ref[...]
    rows = jnp.concatenate([piece, spread_rows(dec_ref[...], piece.shape[0])], 0)
    total = jnp.zeros((rows.shape[0], w_ref.shape[1]), F32)
    for copy, part in zip(copies[small:], parts):
        copy.wait()
        total = total + dot(rows[:, part], w_ref[part, :])
    latent = rms_scale(total, gain_ref[...]).astype(BF16)
    out_ref[...] = latent[: piece.shape[0]]
    dec_out_ref[...] = latent[piece.shape[0] :]


def turn_weights(nope, w_ref, nope_out_ref, rope_out_ref):
    heads = w_ref.shape[0]
    middle = (nope + w_ref.shape[1]) // 2
    per = GROUP // nope
    w_nope = [w_ref[h, :nope, :] for h in range(heads)]
    rotary = []
    for g in range(heads // per):
        mine = range(g * per, (g + 1) * per)
        rotary += [w_ref[h, nope:, :] for h in mine]
        for h in mine:
            rotary += [w_ref[h, middle:, :], w_ref[h, nope:middle, :]]
    nope_out_ref[...] = jnp.concatenate(w_nope, 0).T
    rope_out_ref[...] = jnp.concatenate(rotary, 0).T


def keys_kernel(
    context,
    nope,
    lengths_ref,
    piece_ref,
    dec_ref,
    w_ref,
    w_rope_ref,
    gain_ref,
    cos_ref,
    sin_ref,
    freq_ref,
    prompt_ref,
    w_kup_ref,
    w_vup_ref,
    w_query_ref,
    latent_ref,
    dec_latent_ref,
    rope_ref,
    dec_rope_ref,
    key_ref,
    value_ref,
    new_key_ref,
    new_value_ref,
    w_nope_ref,
    w_turned_ref,
):
    turn_weights(nope, w_query_ref, w_nope_ref, w_turned_ref)
    count = piece_ref.shape[0]
    rope = w_rope_ref.shape[0]
    piece = piece_ref[...]
    rows = jnp.concatenate([piece, spread_rows(dec_ref[...], count)], 0)
    latent = rms_scale(dot(rows, w_ref[...]), gain_ref[...]).astype(BF16)
    w_rope = jnp.concatenate([w_rope_ref[...]] * (LANES // rope), 0)
    raw = dot_nt(rows, w_rope)
    index = lax.axis_index("kv")
    own = pl.ds(pl.multiple_of(index * count, count), count)
    new_rope = turn(raw[:count], cos_ref[own, :], sin_ref[own, :], rope).astype(BF16)
    angle = lengths_ref[...] * freq_ref[...]
    sign = jnp.where(lane_index(angle.shape) % rope < rope // 2, -1.0, 1.0)
    dec_rope = turn(raw[count:], jnp.cos(angle), jnp.sin(angle) * sign, rope).astype(BF16)
    latent_ref[...] = latent[:count]
    dec_latent_ref[...] = latent[count:]
    rope_ref[...] = new_rope
    dec_rope_ref[...] = dec_rope
    w_kup, w_vup = w_kup_ref[...], w_vup_ref[...]
    prompt = prompt_ref[...]
    key_ref[...] = dot_nt(w_kup, prompt).astype(BF16)
    value_ref[...] = dot_nt(prompt, w_vup).astype(BF16)
    new_key_ref[...] = dot_nt(latent[:count], w_kup).astype(BF16)
    new_value_ref[...] = padded(dot_nt(latent[:count], w_vup).astype(BF16))


def split_query_weights(w_ref, nope):
    heads = w_ref.shape[0]
    w_nope = jnp.concatenate([w_ref[h, :nope, :] for h in range(heads)], 0)
    w_rope = jnp.concatenate([w_ref[h, nope:, :] for h in range(heads)], 0)
    return w_nope, w_rope


def attend_kernel(slots, nope, count, *refs):
    (
        w_nope_ref,
        w_rope_ref,
        key_ref,
        value_ref,
        new_key_ref,
        new_value_ref,
        new_rope_ref,
        rope_ref,
        cos_ref,
        sin_ref,
    ) = refs[:10]
    index = lax.axis_index("kv")
    part = lax.axis_index("tp")
    if slots:
        shards = len(slots)
        latent_refs, out_refs, out_ref = refs[10 : 10 + shards], refs[10 + shards : -1], refs[-1]
    else:
        latent_refs, out_ref = refs[10:-1], refs[-1]
    heads = w_nope_ref.shape[1] // nope
    rope = rope_ref.shape[0]
    latents = jnp.concatenate([ref[...] for ref in latent_refs], 0)
    if slots:
        owners = [lax.rem(index - pick(part, steps) + shards, shards) for steps in slots]
    else:
        first = pl.program_id(0) * (latents.shape[0] // count)
        owners = [first + s for s in range(latents.shape[0] // count)]
    queries = latents.shape[0]
    tables = [pl.ds(pl.multiple_of(owner * count, count), count) for owner in owners]
    cosine = jnp.concatenate([cos_ref[part, :] for part in tables], 0)
    sine = jnp.concatenate([sin_ref[part, :] for part in tables], 0)
    scale = (nope + rope) ** (-0.5)
    per, pair = GROUP // nope, LANES // nope
    old_rope = jnp.concatenate([rope_ref[...]] * (LANES // rope), 0)
    new_rope = new_rope_ref[...]
    row = row_index((count, LANES))
    column = lane_index((count, LANES))
    allowed = jnp.concatenate(
        [
            (column < count) & (index * count + column <= owner * count + row)
            for owner in owners
        ]
        * pair,
        0,
    )
    lane = lane_index((queries, LANES))
    rate = scale * LOG2_E
    stats = jnp.zeros((queries, LANES), F32)
    tiles = key_ref.shape[1] // LANES
    ropes, nopes = [], []
    for g in range(heads // per):
        wide = slice(g * GROUP, (g + 1) * GROUP)
        q_rope = dot(latents, w_rope_ref[:, wide])
        ropes.append(q_rope[:, :LANES] * cosine + q_rope[:, LANES:] * sine)
        nopes.append(dot(latents, w_nope_ref[:, wide]).astype(BF16).astype(F32))
    scores = []
    for first in range(0, heads, pair):
        g, p = first // per, first % per // pair
        narrow = slice(first * nope, first * nope + LANES)
        rows = slice(p * pair * queries, (p + 1) * pair * queries)
        query = jnp.concatenate(
            [
                diagonal(nopes[g][:, p * LANES : (p + 1) * LANES], pair, nope),
                diagonal(ropes[g], per, rope)[rows],
            ],
            1,
        ).astype(BF16)
        old = dot(query, jnp.concatenate([key_ref[narrow, :], old_rope], 0))
        new = dot_nt(query, jnp.concatenate([new_key_ref[:, narrow], new_rope], 1))
        empty = jnp.zeros((new.shape[0], LANES - count), F32)
        new = jnp.where(allowed, jnp.concatenate([new, empty], 1), -1e30)
        scores.append([old[:, t * LANES : (t + 1) * LANES] for t in range(tiles)] + [new])
    weights = []
    for number, pieces in enumerate(scores):
        top = jnp.max(functools.reduce(jnp.maximum, pieces), axis=-1, keepdims=True)
        pieces = [jnp.exp2((piece - top) * rate) for piece in pieces]
        total = jnp.sum(sum(pieces), axis=-1, keepdims=True)
        weights.append([piece.astype(BF16) for piece in pieces])
        for j in range(pair):
            own = slice(j * queries, (j + 1) * queries)
            stats = jnp.where(
                lane % heads == number * pair + j,
                jnp.where(lane < 3 * heads, top[own] * scale, total[own]),
                stats,
            )
    for g in range(heads // per):
        wide = slice(g * GROUP, (g + 1) * GROUP)
        mine = weights[g * per // pair : (g + 1) * per // pair]
        old = jnp.concatenate([jnp.concatenate(pieces[:-1], 1) for pieces in mine], 0)
        new = jnp.concatenate([pieces[-1] for pieces in mine], 0)
        mixed = dot(old, value_ref[:, wide]) + dot(new, new_value_ref[:, wide])
        owner_lane = lane_index((queries, GROUP)) // nope
        kept = jnp.zeros((queries, GROUP), F32)
        for j in range(per):
            kept = jnp.where(owner_lane == j, mixed[j * queries : (j + 1) * queries], kept)
        out_ref[:, wide] = kept.astype(BF16)
    high = stats.astype(BF16).astype(F32)
    rest = stats - high
    middle = rest.astype(BF16).astype(F32)
    piece = (lane // heads) % 3
    stats = jnp.where(piece == 0, high, jnp.where(piece == 1, middle, rest - middle))
    stats = jnp.where(lane < 6 * heads, stats, 0.0)
    out_ref[:, heads * nope :] = stats.astype(BF16)
    if slots:
        for back, ref in enumerate(out_refs):
            places = [[steps[t] for steps in slots].index(back) for t in range(len(slots[0]))]
            ref[...] = block_at(out_ref, pick(part, places), count)


def decode_kernel(
    nope,
    lengths_ref,
    q_ref,
    w_ref,
    w_kup_ref,
    w_vup_ref,
    latent_ref,
    rope_ref,
    new_latent_ref,
    new_rope_ref,
    freq_ref,
    piece_latent_ref,
    piece_rope_ref,
    out_ref,
    latent_out_ref,
    dec_latent_out_ref,
    rope_out_ref,
    dec_rope_out_ref,
):
    heads = w_ref.shape[0]
    rope = w_ref.shape[1] - nope
    latent_out_ref[...] = piece_latent_ref[...]
    dec_latent_out_ref[...] = new_latent_ref[:1, :]
    rope_out_ref[...] = piece_rope_ref[: rope_out_ref.shape[0], :rope]
    dec_rope_out_ref[...] = new_rope_ref[:1, :rope]
    length = lengths_ref[...]
    scale = (nope + rope) ** (-0.5)
    latents = q_ref[...]
    rows = latents.shape[0]
    w_nope, w_rope = split_query_weights(w_ref, nope)
    q_nope = dot_nt(latents, w_nope)
    q_rope = dot_nt(latents, w_rope)
    angle = length * freq_ref[...]
    sign = jnp.where(lane_index(angle.shape) % rope < rope // 2, -1.0, 1.0)
    cosine, sine = jnp.cos(angle), jnp.sin(angle) * sign
    shape = q_nope.shape
    spread = jnp.where(lane_index(shape) // nope == row_index(shape), q_nope, 0.0).astype(BF16)
    absorbed = dot(spread, w_kup_ref[...]).astype(BF16)
    turned = jnp.concatenate(
        [
            turn(q_rope[:, t * LANES : (t + 1) * LANES], cosine, sine, rope)
            for t in range(heads * rope // LANES)
        ],
        1,
    )
    shape = turned.shape
    own_lane = lane_index(shape) // rope == row_index(shape)
    spread_rope = jnp.where(own_lane, turned, 0.0).astype(BF16)
    rope_keys = jnp.concatenate([rope_ref[...]] * heads, 0)
    cached = (dot_nt(absorbed, latent_ref[...]) + dot(spread_rope, rope_keys)) * scale
    cached = jnp.where(lane_index(cached.shape).astype(F32) < length[:, :1], cached, -1e30)
    new_latent = new_latent_ref[...].astype(F32)
    new_rope = jnp.concatenate([new_rope_ref[...].astype(F32)] * (heads * rope // LANES), 1)
    own = (
        jnp.sum(absorbed.astype(F32) * new_latent, axis=-1, keepdims=True)
        + jnp.sum(spread_rope.astype(F32) * new_rope, axis=-1, keepdims=True)
    ) * scale
    top = jnp.maximum(jnp.max(cached, axis=-1, keepdims=True), own)
    cached = jnp.exp(cached - top)
    own = jnp.exp(own - top)
    total = jnp.sum(cached, axis=-1, keepdims=True) + own
    own = (own / total).astype(BF16).astype(F32)
    context = dot((cached / total).astype(BF16), latent_ref[...]) + own * new_latent
    mixed = dot_nt(context.astype(BF16), w_vup_ref[...])
    shape = mixed.shape
    value_dim = w_vup_ref.shape[0] // heads
    mixed = jnp.where(lane_index(shape) // value_dim == row_index(shape), mixed, 0.0)
    total = jnp.sum(mixed, axis=0, keepdims=True)
    out_ref[...] = jnp.broadcast_to(total, out_ref.shape).astype(BF16)


def combine_kernel(heads, dec_ref, w_ref, chosen_ref, *refs):
    count = dec_ref.shape[0]
    got, out_ref = [ref[...] for ref in refs[:-1]], refs[-1]
    width = w_ref.shape[0]
    tails = dot(jnp.concatenate([block[:, width:] for block in got], 0), chosen_ref[...])
    tops = [tails[b * count : (b + 1) * count, :width] for b in range(len(got))]
    totals = [tails[b * count : (b + 1) * count, width:] for b in range(len(got))]
    best = functools.reduce(jnp.maximum, tops)
    factors = [jnp.exp(top - best) for top in tops]
    total = sum(factor * total for factor, total in zip(factors, totals))
    mixed = sum(block[:, :width].astype(F32) * factor for block, factor in zip(got, factors))
    rows = jnp.concatenate([(mixed / total).astype(BF16), dec_ref[...]], 0)
    out_ref[...] = dot(rows, w_ref[...])[: out_ref.shape[0]].astype(BF16)


def chosen_lanes(heads, value_dim):
    lane = np.arange(LANES)[:, None]
    head = np.arange(heads * value_dim)[None, :] // value_dim
    same = lane % heads == head
    tops, totals = same & (lane < 3 * heads), same & (lane >= 3 * heads) & (lane < 6 * heads)
    return np.concatenate([tops, totals], 1).astype(np.float32)


def add_kernel(*refs):
    term_refs, piece_ref, dec_ref = refs[:-2], refs[-2], refs[-1]
    total = sum(ref[...].astype(F32) for ref in term_refs)
    count = piece_ref.shape[0]
    piece_ref[...] = total[:count].astype(BF16)
    dec_ref[...] = total[count : count + 1].astype(BF16)


def call(kernel, outs, in_specs, name, flops, **extra):
    many = isinstance(outs, list)
    shapes = []
    for out in outs if many else [outs]:
        shapes.append(jax.ShapeDtypeStruct(out, BF16))
    limit = extra.pop("limit", 8 << 20)
    specs = [VMEM] * len(shapes)
    return pl.pallas_call(
        kernel,
        out_shape=shapes if many else shapes[0],
        in_specs=in_specs,
        out_specs=specs if many else specs[0],
        name=name,
        compiler_params=pltpu.CompilerParams(vmem_limit_bytes=limit),
        cost_estimate=pl.CostEstimate(flops=flops, bytes_accessed=flops // 64, transcendentals=0),
        **extra,
    )


def ring_pairs(shards, step):
    return [(i, (i + step) % shards) for i in range(shards)]


def mixed_pairs(shards, parts, taken):
    return [
        (i * parts + t, (i + taken[t % len(taken)]) % shards * parts + t)
        for i in range(shards)
        for t in range(parts)
    ]


def swap(values, axis, step):
    return lax.ppermute(values, axis, ring_pairs(lax.axis_size(axis), step))


def gather_plan(shards, parts):
    steps = list(range(1, shards))
    plan = []
    while steps:
        together = parts if parts == 2 and len(steps) >= 2 else 1
        plan.append(steps[:together])
        steps = steps[together:]
    return plan


def slot_steps(plan, parts):
    slots = [[0] * parts]
    for taken in plan:
        for turned in range(len(taken)):
            slots.append([taken[(t + turned) % len(taken)] for t in range(parts)])
    return slots


def pick(index, values):
    chosen = jnp.int32(values[0])
    for i, value in enumerate(values):
        if value != values[0]:
            chosen = jnp.where(index == i, value, chosen)
    return chosen


def block_at(ref, number, count):
    return ref[pl.ds(pl.multiple_of(number * count, count), count), :]


def in_hbm(array):
    return pltpu.with_memory_space_constraint(array, pltpu.HBM)


def rope_tables(context, rows, rope):
    half = rope // 2
    inverse = ROPE_BASE ** (-np.arange(half, dtype=np.float32) * 2.0 / rope)
    inverse = inverse.astype(np.float32)
    lanes = np.tile(inverse, LANES // half)[None, :]
    angle = (context + np.arange(rows, dtype=np.float32))[:, None] * lanes
    sign = np.where(np.arange(LANES) % rope < half, -1.0, 1.0)
    return (
        np.cos(angle).astype(np.float32),
        (np.sin(angle) * sign).astype(np.float32),
        lanes.astype(np.float32),
    )


def per_device(
    piece_rows,
    decode_rows,
    prompt_latent,
    prompt_rope_key,
    decode_latent,
    decode_rope_key,
    dec_lengths,
    w_qdown,
    q_gain,
    w_qup,
    w_kvdown,
    w_krope,
    kv_gain,
    w_kup,
    w_vup,
    w_out,
):
    shards, parts = lax.axis_size("kv"), lax.axis_size("tp")
    count, model = piece_rows.shape
    cached, width = prompt_latent.shape
    context = cached * shards
    heads, nope = w_kup.shape[1:]
    value_dim = w_vup.shape[2]
    rope = w_krope.shape[1]
    assert decode_rows.shape[0] == 1
    cosine, sine, freq = rope_tables(context, count * shards, rope)
    w_query = jnp.transpose(w_qup, (1, 2, 0))
    w_key = jnp.transpose(w_kup, (1, 2, 0)).reshape(heads * nope, width)
    w_value = jnp.transpose(w_vup, (1, 2, 0)).reshape(heads * value_dim, width)
    w_last = w_out.reshape(heads * value_dim, model)
    packed_width = heads * value_dim + LANES

    q_latent, q_decode = call(
        query_latent_kernel,
        [(count, w_qdown.shape[1]), (count, w_qdown.shape[1])],
        [HBM] * 4,
        "query_latent",
        2 * 2 * count * model * w_qdown.shape[1] * 100,
        scratch_shapes=[
            pltpu.VMEM(piece_rows.shape, BF16),
            pltpu.VMEM(decode_rows.shape, BF16),
            pltpu.VMEM((1, q_gain.shape[0]), F32),
            pltpu.VMEM(w_qdown.shape, BF16),
            pltpu.SemaphoreType.DMA((len(CUTS) - 1 + 3,)),
        ],
    )(*[in_hbm(array) for array in (piece_rows, decode_rows, w_qdown, q_gain[None, :])])

    length = jnp.broadcast_to(dec_lengths.astype(F32)[:, None], (1, LANES))
    direct = shards <= MAX_PERMUTES
    if direct:
        plan = gather_plan(shards, parts)
        slots = slot_steps(plan, parts)
        blocks = [q_latent]
        for taken in plan:
            blocks.append(lax.ppermute(q_latent, ("kv", "tp"), mixed_pairs(shards, parts, taken)))
            if len(taken) > 1:
                blocks.append(swap(blocks[-1], "tp", 1))
    else:
        blocks = [lax.all_gather(q_latent, "kv", axis=0, tiled=True)]

    (
        new_latent,
        dec_latent_rows,
        new_rope,
        dec_rope_rows,
        keys,
        values,
        new_keys,
        new_values,
        w_nope,
        w_rope,
    ) = call(
        functools.partial(keys_kernel, context, nope),
        [
            (count, width),
            (count, width),
            (count, LANES),
            (count, LANES),
            (heads * nope, cached),
            (cached, heads * value_dim),
            (count, heads * nope),
            (LANES, heads * value_dim),
            (w_qup.shape[0], heads * nope),
            (w_qup.shape[0], heads * rope * 2),
        ],
        [VMEM] * 13,
        "keys",
        4 * cached * width * heads * nope,
    )(
        length,
        piece_rows,
        decode_rows,
        w_kvdown,
        w_krope.T,
        kv_gain[None, :],
        cosine,
        sine,
        freq,
        prompt_latent,
        w_key,
        w_value,
        w_query,
    )

    shared = (
        w_nope,
        w_rope,
        keys,
        values,
        new_keys,
        new_values,
        new_rope,
        prompt_rope_key.T,
        cosine,
        sine,
    )
    total_rows = count * shards
    flops = 4 * total_rows * cached * heads * nope
    if direct:
        sent = call(
            functools.partial(attend_kernel, slots, nope, count),
            [(count, packed_width)] * shards,
            [VMEM] * (len(shared) + shards),
            "attend",
            flops,
            scratch_shapes=[pltpu.VMEM((total_rows, packed_width), BF16)],
        )(*shared, *blocks)
        got = [sent[0]] + [swap(sent[shards - s], "kv", s) for s in range(1, shards)]
    else:
        step_rows = min(64, total_rows)
        whole = [
            pl.BlockSpec(array.shape, lambda i, rank=array.ndim: (0,) * rank) for array in shared
        ]
        packed = pl.pallas_call(
            functools.partial(attend_kernel, None, nope, count),
            grid=(total_rows // step_rows,),
            out_shape=jax.ShapeDtypeStruct((total_rows, packed_width), BF16),
            in_specs=whole + [pl.BlockSpec((step_rows, w_qdown.shape[1]), lambda i: (i, 0))],
            out_specs=pl.BlockSpec((step_rows, packed_width), lambda i: (i, 0)),
            name="attend",
            compiler_params=pltpu.CompilerParams(vmem_limit_bytes=24 << 20),
        )(*shared, *blocks)
        got = lax.all_to_all(packed, "kv", split_axis=0, concat_axis=0, tiled=True)
        got = [got[s * count : (s + 1) * count] for s in range(shards)]

    dec_heads, piece_latent, dec_latent, piece_rope, dec_rope = call(
        functools.partial(decode_kernel, nope),
        [(count, heads * value_dim), (count, width), (1, width), (count, rope), (1, rope)],
        [VMEM] * 12,
        "decode",
        4 * count * decode_latent.shape[1] * width * 4,
    )(
        length,
        q_decode,
        w_query,
        w_key,
        w_value,
        decode_latent[0],
        decode_rope_key[0].T,
        dec_latent_rows,
        dec_rope_rows,
        freq,
        new_latent,
        new_rope,
    )

    term = call(
        functools.partial(combine_kernel, heads),
        (count + 8, model),
        [VMEM] * (3 + len(got)),
        "combine",
        2 * 2 * count * heads * value_dim * model,
    )(dec_heads, w_last, jnp.asarray(chosen_lanes(heads, value_dim), BF16), *got)
    terms = [term] + [swap(term, "tp", s) for s in range(1, parts)]
    piece_out, decode_out = call(
        add_kernel, [(count, model), (1, model)], [VMEM] * len(terms), "add", 1000
    )(*terms)
    return (piece_out, decode_out, piece_latent, piece_rope, dec_latent, dec_rope)


def solution(mesh):
    rows = P(("dp", "kv"), None)
    cube = P(("dp", "kv"), None, None)
    by_head = P(None, "tp", None)
    in_specs = (
        rows,
        rows,
        rows,
        rows,
        cube,
        cube,
        P(("dp", "kv")),
        P(),
        P(),
        by_head,
        P(),
        P(),
        P(),
        by_head,
        by_head,
        P("tp", None, None),
    )
    return jax.shard_map(
        per_device, mesh=mesh, in_specs=in_specs, out_specs=(rows,) * 6, check_vma=False
    )
```
